32 devices in a mesh: sp: 4 (over y, x), tp: 8 (over z, core).
Axes of the slice: x: 2, y: 2, z: 4, core: 2. Of those that a mesh axis runs over, the one named last changes fastest.
Arguments:
- inputs: bfloat16 [2, 2048, 4096], P(None, 'sp', 'tp'), may hold values from -16 to 16
- in_gain: float32 [4096], replicated, may hold values from 0.1 to 1.9
- key_weight: bfloat16 [4096, 2048], P(None, 'tp'), may hold values from -0.0014648438 to 0.0014648438
- value_weight: bfloat16 [4096, 4096], P(None, 'tp'), may hold values from -0.09375 to 0.09375
- decay_down: bfloat16 [4096, 32], replicated, may hold values from -0.09375 to 0.09375
- decay_up: bfloat16 [32, 2048], replicated, may hold values from -1 to 1
- decay_bias: float32 [2048], replicated, may hold values from 0 to 10
- new_query: bfloat16 [2, 2048], P(None, 'tp'), may hold values from -6 to 6
- out_gain: float32 [256], replicated, may hold values from 0.1 to 1.9
Outputs:
- cache: bfloat16 [2, 16, 128, 256], P(None, 'tp', 'sp')
- read: bfloat16 [2, 4096], P(None, 'tp')
The draws below stay inside these ranges and needn't reach their ends.
All inputs are finite; a program needn't handle non-finite values.
Results may differ from the reference program's by a relative error of at most 0.0085.
Values may be sent and summed in bfloat16 or wider, within the bound.
A program may use at most 64 MiB of HBM per device.

```python
import jax
import jax.numpy as jnp
from jax import lax

D = 4096
HEADS = 16
DK = 128
DV = 256
RANK = 32
SEQS = 2
SPAN_DEV = 512
SEQ_LEN = 2048


def draw_inputs(key, part):
    jitter_key, shared_key, level_key = jax.random.split(key, 3)
    run_length = max(SPAN_DEV // 2, 1)
    run_count = SEQ_LEN // run_length
    jitter = jax.random.normal(jitter_key, (SEQS, SEQ_LEN, D), jnp.float32)
    levels = jax.random.uniform(level_key, (16,), jnp.float32, -1.1, 1.1)
    shared = jax.random.normal(shared_key, (SEQS, run_count, D), jnp.float32)
    shared = jnp.repeat(shared, run_length, axis=1)
    factor = jnp.repeat(jnp.exp(levels), D // 16)
    return jnp.clip((jitter + 0.5 * shared) * factor, -16.0, 16.0).astype(jnp.bfloat16)


def draw_decay_bias(key, part):
    pick_key, slow_key, quick_key = jax.random.split(key, 3)
    share_slow = 0.5
    chosen = jax.random.uniform(pick_key, (HEADS * DK,), jnp.float32) < share_slow
    slow_bias = jax.random.uniform(slow_key, (HEADS * DK,), jnp.float32, 5.5, 7.0)
    quick_bias = jax.random.uniform(quick_key, (HEADS * DK,), jnp.float32, 0.0, 1.5)
    return jnp.where(chosen, slow_bias, quick_bias)


def block_levels(stream_key, dims, pieces, least, top_value):
    gain = 1.0
    for position, shards_of in pieces:
        heights = jax.random.uniform(jax.random.fold_in(jax.random.fold_in(stream_key, 6), position), (shards_of,), jnp.float32, least / len(pieces), top_value / len(pieces))
        gain = gain * jnp.repeat(jnp.exp(heights), dims[position] // shards_of).reshape((-1,) + (1,) * (len(dims) - 1 - position))
    return gain


def gaussian(stream_key, dims, scale, bound, pieces=(), held_as=jnp.bfloat16):
    result = jax.random.normal(stream_key, dims, jnp.float32) * scale
    if len(pieces) > 0:
        result = block_levels(stream_key, dims, pieces, -0.22, 0.18) * result
    return jnp.clip(result, min=-bound, max=bound).astype(held_as)


def setup_inputs(seed: int = 0) -> dict:
    arg_keys = jax.random.split(jax.random.key(seed), 10)
    inputs = draw_inputs(jax.random.fold_in(arg_keys[9], 71), 0)
    in_gain = jnp.clip(1.0 + 0.18 * jax.random.normal(arg_keys[1], (D,), jnp.float32), 0.1, 1.9)
    key_weight = gaussian(arg_keys[2], (D, HEADS * DK), (D * 4096) ** -0.5, 0.0014648438, ((1, 8),))
    value_weight = gaussian(arg_keys[3], (D, HEADS * DV), D ** -0.5, 0.09375, ((1, 8),))
    decay_down = gaussian(arg_keys[4], (D, RANK), D ** -0.5, 0.09375)
    decay_up = gaussian(arg_keys[5], (RANK, HEADS * DK), RANK ** -0.5, 1.0)
    decay_bias = draw_decay_bias(jax.random.fold_in(arg_keys[9], 71), 0)
    new_query = gaussian(arg_keys[7], (SEQS, HEADS * DK), 1.0, 6.0, ((1, 8),))
    out_gain = jnp.clip(1.0 + 0.18 * jax.random.normal(arg_keys[8], (DV,), jnp.float32), 0.1, 1.9)
    return dict(inputs=inputs, in_gain=in_gain, key_weight=key_weight, value_weight=value_weight, decay_down=decay_down, decay_up=decay_up, decay_bias=decay_bias, new_query=new_query, out_gain=out_gain)


def reference(inputs, in_gain, key_weight, value_weight, decay_down, decay_up, decay_bias, new_query, out_gain):
    scaled = (inputs * in_gain).astype(jnp.bfloat16)
    widened = inputs.astype(jnp.float32)
    inv_rms = lax.rsqrt(lax.optimization_barrier(jnp.mean(widened * widened, axis=-1)) + 1e-06).reshape(-1, 1)
    flat_rows = scaled.reshape(-1, D)
    key_rows = (jnp.dot(flat_rows, key_weight, preferred_element_type=jnp.float32) * inv_rms).astype(jnp.bfloat16)
    value_rows = (jnp.dot(flat_rows, value_weight, preferred_element_type=jnp.float32) * inv_rms).astype(jnp.bfloat16)
    low_rank = jnp.dot(flat_rows, decay_down, preferred_element_type=jnp.float32) * inv_rms
    gate_pre = jnp.dot(low_rank, decay_up.astype(jnp.float32), precision=lax.Precision.HIGHEST) + decay_bias
    log_decay = jax.nn.log_sigmoid(gate_pre) / 16.0
    block_count = SEQ_LEN // SPAN_DEV
    log_decay = log_decay.reshape(SEQS, block_count, SPAN_DEV, HEADS, DK)
    inclusive = jnp.cumsum(log_decay, axis=2)
    block_total = inclusive[:, :, -1]
    suffix = block_total[:, :, None] - inclusive
    weighted = (key_rows.reshape(SEQS, block_count, SPAN_DEV, HEADS, DK).astype(jnp.float32) * jnp.exp(suffix)).astype(jnp.bfloat16)
    block_state = jnp.einsum('sbthk,sbthv->sbhkv', weighted.astype(jnp.float32), value_rows.reshape(SEQS, block_count, SPAN_DEV, HEADS, DV).astype(jnp.float32))
    running = jnp.cumsum(block_total, axis=1)
    later_sum = running[:, -1:] - running
    state = jnp.einsum('sbhk,sbhkv->shkv', jnp.exp(later_sum), block_state)
    cache = state.astype(jnp.bfloat16)
    readout = jnp.einsum('shk,shkv->shv', new_query.reshape(SEQS, HEADS, DK).astype(jnp.float32), cache.astype(jnp.float32))
    normed = readout * lax.rsqrt(lax.optimization_barrier(jnp.mean(readout * readout, axis=-1, keepdims=True)) + 1e-06) * out_gain
    return (cache, normed.astype(jnp.bfloat16).reshape(SEQS, HEADS * DV))
```

```python
import functools

import jax
import jax.numpy as jnp
from jax import lax
from jax.experimental import pallas as pl
from jax.experimental.pallas import tpu as pltpu
from jax.sharding import PartitionSpec as P

DK = 128
DV = 256
CHUNK = 128
LENT_SEQ = 0
MESH = pl.DeviceIdType.MESH
F32 = jnp.float32
BF16 = jnp.bfloat16


def split3(value):
    high = value.astype(BF16)
    rest = value - high.astype(F32)
    middle = rest.astype(BF16)
    low = (rest - middle.astype(F32)).astype(BF16)
    return high, middle, low


def lends(n_sp, n_z, heads):
    return n_z >= 4 and n_sp == 2 * heads


def kernel(
    n_sp,
    n_z,
    x_ref,
    gain_hbm,
    wk_hbm,
    wv_hbm,
    wd_hbm,
    up_hbm,
    bias_hbm,
    query_hbm,
    cache_ref,
    parts_ref,
    xbuf,
    wk,
    wv,
    wd,
    up,
    bias,
    gain_ref,
    query_ref,
    acc_k,
    acc_v,
    acc_l,
    acc_s,
    state,
    carry,
    fade,
    scale,
    tots,
    terms,
    landed,
    reads,
    load_sem,
    own_sem,
    hop_send,
    pair_send,
    recv,
    tot_send,
    tot_recv,
    term_send,
    term_recv,
    read_send,
    read_recv,
    lent_x=None,
    lent_wk=None,
    lent_wv=None,
    lent_up=None,
    lent_bias=None,
    lent_k=None,
    lent_v=None,
    lent_l=None,
    lent_s=None,
    lent_fade=None,
    lent_scale=None,
    hint=None,
    lent_terms=None,
    lent_tots=None,
    back_terms=None,
    back_tots=None,
    hint_send=None,
    hint_recv=None,
    lent_x_send=None,
    lent_x_recv=None,
    lent_w_send=None,
    lent_w_pair=None,
    lent_w_recv=None,
    back_send=None,
    back_recv=None,
):
    seqs, span, feats = x_ref.shape
    per_seq = span // CHUNK
    chunks = seqs * per_seq
    heads = wk_hbm.shape[1] // DK
    share = DK // n_sp
    slots = 2 * n_z
    model = slots * feats
    lend = lends(n_sp, n_z, heads)
    lent = LENT_SEQ * per_seq + per_seq - 1
    tail = chunks - 1
    sp = lax.axis_index("sp")
    tp = lax.axis_index("tp")
    z = tp // 2
    c = lax.rem(tp, 2)
    key_cols = heads * DK
    at_end = (z == 0) | (z == n_z - 1)
    low_half = z < n_z // 2
    end = jnp.where(low_half, 0, n_z - 1)
    inner = jnp.where(low_half, 1, n_z - 2)
    at_inner = z == inner
    flip = jnp.where(low_half, 1, -1)
    reach = jnp.where(low_half, n_z - 1 - z, z)
    final_step = 2 * reach - 1
    lender = at_end & (c == sp // 2)
    peers = [lax.rem(sp + off, n_sp) for off in range(1, n_sp)]

    first = pl.multiple_of(tp * key_cols, key_cols)
    loads = [
        pltpu.make_async_copy(wk_hbm, wk, load_sem.at[0]),
        pltpu.make_async_copy(wv_hbm, wv, load_sem.at[1]),
        pltpu.make_async_copy(wd_hbm, wd, load_sem.at[2]),
        pltpu.make_async_copy(up_hbm.at[:, pl.ds(first, key_cols)], up, load_sem.at[3]),
        pltpu.make_async_copy(bias_hbm.at[:, pl.ds(first, key_cols)], bias, load_sem.at[4]),
        pltpu.make_async_copy(gain_hbm, gain_ref, load_sem.at[5]),
        pltpu.make_async_copy(query_hbm, query_ref, load_sem.at[6]),
    ]
    if lend:
        other = pl.multiple_of((end * 2 * heads + sp) * DK, DK)
        loads += [
            pltpu.make_async_copy(up_hbm.at[:, pl.ds(other, DK)], lent_up, load_sem.at[7]),
            pltpu.make_async_copy(bias_hbm.at[:, pl.ds(other, DK)], lent_bias, load_sem.at[8]),
        ]

    def stage_w(act):
        head = lax.rem(sp, 2)
        for n, (src, dst, width) in enumerate(((wk_hbm, lent_wk, DK), (wv_hbm, lent_wv, DV))):
            columns = pl.ds(pl.multiple_of(head * width, width), width)
            act(pltpu.make_async_copy(src.at[:, columns], dst, load_sem.at[9 + n]))

    def chunk_rows(j):
        seq = j // per_seq
        start = (per_seq - 1 - lax.rem(j, per_seq)) * CHUNK
        return seq, pl.multiple_of(start, CHUNK)

    def own_copy(j):
        seq, start = chunk_rows(j)
        return pltpu.make_async_copy(
            x_ref.at[seq, pl.ds(start, CHUNK), :], xbuf.at[j, z, c], own_sem.at[j]
        )

    def hop_copy(j, zz, way):
        return pltpu.make_async_remote_copy(
            src_ref=xbuf.at[j, zz, c],
            dst_ref=xbuf.at[j, zz, c],
            send_sem=hop_send.at[j, zz, way],
            recv_sem=recv.at[j, zz, c],
            device_id={"tp": (z + 2 * way - 1) * 2 + c},
            device_id_type=MESH,
        )

    def pair_copy(j, zz, cc):
        return pltpu.make_async_remote_copy(
            src_ref=xbuf.at[j, zz, cc],
            dst_ref=xbuf.at[j, zz, cc],
            send_sem=pair_send.at[j, zz],
            recv_sem=recv.at[j, zz, cc],
            device_id={"tp": tp + 1 - 2 * c},
            device_id_type=MESH,
        )

    def each_way(j, zz, act):
        for way, edge in ((0, 0), (1, n_z - 1)):
            there = z + 2 * way - 1
            beyond = (zz >= z) if way == 0 else (zz <= z)
            wanted = (z != edge) & beyond
            if lend:
                wanted = wanted & ((j != lent) | (there != edge))

            @pl.when(wanted)
            def _():
                act(hop_copy(j, zz, way))

    def held(j, zz):
        return at_inner & (j == tail) & (flip * (zz - z) > 0)

    def used(j):
        if not lend:
            return j >= 0
        return (j != lent) | jnp.logical_not(at_end)

    def lend_x(zz, act):
        for n, peer in enumerate(peers):
            act(
                pltpu.make_async_remote_copy(
                    src_ref=xbuf.at[lent, zz, c],
                    dst_ref=lent_x.at[lax.rem(sp, 2), zz, c],
                    send_sem=lent_x_send.at[zz, n],
                    recv_sem=lent_x_recv.at[lax.rem(sp, 2), zz, c],
                    device_id={"sp": peer, "tp": z * 2 + sp // 2},
                    device_id_type=MESH,
                )
            )

    def lend_w(slot, act):
        rows = pl.ds(pl.multiple_of(slot * feats, feats), feats)
        for n, both in enumerate((lent_wk, lent_wv)):
            act(
                pltpu.make_async_remote_copy(
                    src_ref=both.at[rows, :],
                    dst_ref=both.at[rows, :],
                    send_sem=lent_w_send.at[n, slot],
                    recv_sem=lent_w_recv.at[n, slot],
                    device_id={"tp": inner * 2 + c},
                    device_id_type=MESH,
                )
            )

    def pair_w(slot, act):
        rows = pl.ds(pl.multiple_of(slot * feats, feats), feats)
        for n, both in enumerate((lent_wk, lent_wv)):
            act(
                pltpu.make_async_remote_copy(
                    src_ref=both.at[rows, :],
                    dst_ref=both.at[rows, :],
                    send_sem=lent_w_pair.at[n, slot],
                    recv_sem=lent_w_recv.at[n, slot],
                    device_id={"tp": tp + 1 - 2 * c},
                    device_id_type=MESH,
                )
            )

    def hint_copy():
        return pltpu.make_async_remote_copy(
            src_ref=hint,
            dst_ref=hint,
            send_sem=hint_send,
            recv_sem=hint_recv,
            device_id={"tp": end * 2 + c},
            device_id_type=MESH,
        )

    def give_back(n, p):
        lines = pl.ds(2 * c, 2)
        src, dst = ((lent_tots, back_tots), (lent_terms.at[p], back_terms))[n]
        return pltpu.make_async_remote_copy(
            src_ref=src,
            dst_ref=dst.at[lax.rem(sp, 2), lines],
            send_sem=back_send.at[n, p],
            recv_sem=back_recv.at[n, lax.rem(sp, 2), c],
            device_id={"sp": p, "tp": end * 2 + sp // 2},
            device_id_type=MESH,
        )

    for j in range(chunks):
        own_copy(j).start()
    for load in loads:
        load.start()
    if lend:
        pl.when(lender)(lambda: stage_w(lambda copy: copy.start()))

    barrier = pltpu.get_barrier_semaphore()

    def greet(ahead, device):
        @pl.when(ahead)
        def _():
            pl.semaphore_signal(barrier, inc=1, device_id=device, device_id_type=MESH)

    close = at_end | at_inner if lend else False
    apart = jnp.logical_not(close)
    for way, edge in ((0, 0), (1, n_z - 1)):
        there = z + 2 * way - 1
        met = z != edge
        if lend:
            met = met & jnp.logical_not(close & ((there == end) | (there == inner)))
        greet(met, {"tp": there * 2 + c})
    if lend:
        for p in range(n_sp):
            for plane in (end, inner):
                for core in range(2):
                    known = close & ((p != sp) | (plane != z) | (core != c))
                    greet(known, {"sp": p, "tp": plane * 2 + core})
        greet(apart, {"tp": tp + 1 - 2 * c})
        for peer in peers:
            greet(apart, {"sp": peer})
        far = jnp.where(close, 4 * n_sp - 1 + jnp.where(at_inner, 1, 0), 2 + n_sp)
    else:
        greet(tp >= 0, {"tp": tp + 1 - 2 * c})
        for peer in peers:
            greet(tp >= 0, {"sp": peer})
        far = n_sp + jnp.where(z > 0, 1, 0) + jnp.where(z < n_z - 1, 1, 0)

    acc_k[...] = jnp.zeros_like(acc_k)
    acc_v[...] = jnp.zeros_like(acc_v)
    acc_l[...] = jnp.zeros_like(acc_l)
    acc_s[...] = jnp.zeros_like(acc_s)
    if lend:

        @pl.when(at_inner)
        def _():
            lent_k[...] = jnp.zeros_like(lent_k)
            lent_v[...] = jnp.zeros_like(lent_v)
            lent_l[...] = jnp.zeros_like(lent_l)
            lent_s[...] = jnp.zeros_like(lent_s)

        @pl.when(jnp.logical_not(at_end))
        def _():
            back_terms[...] = jnp.zeros_like(back_terms)
            back_tots[...] = jnp.zeros_like(back_tots)

    pl.semaphore_wait(barrier, far)

    def open_chunk(j, _):
        own_copy(j).wait()
        each_way(j, z, lambda copy: copy.start())

        @pl.when(used(j))
        def _():
            pair_copy(j, z, c).start()

        return 0

    lax.fori_loop(0, chunks, open_chunk, 0)
    if lend:

        @pl.when(at_inner)
        def _():
            lend_x(z, lambda copy: copy.start())

    for load in loads:
        load.wait()
    if lend:
        pl.when(lender)(lambda: stage_w(lambda copy: copy.wait()))

    def project(scaled, slot, rows, weights, accs):
        deep = pl.ds(pl.multiple_of(slot * feats, feats), feats)
        for weight, acc in zip(weights, accs):
            acc[rows] += jnp.dot(scaled, weight[deep, :], preferred_element_type=F32)

    def reduce_rank(wide, scaled, slot, rows, acc_rank, acc_square):
        deep = pl.ds(pl.multiple_of(slot * feats, feats), feats)
        acc_rank[rows] += lax.dot_general(
            scaled, wd[:, deep], (((1,), (1,)), ((), ())), preferred_element_type=F32
        )
        square = wide * wide
        total = square[:, 0:128]
        for lane in range(128, feats, 128):
            total = total + square[:, lane : lane + 128]
        acc_square[rows] += total

    def add_shard(j, zz, cc):
        slot = zz * 2 + cc
        wide = xbuf[j, zz, cc].astype(F32)
        scaled = (wide * gain_ref[slot]).astype(BF16)
        project(scaled, slot, j, (wk, wv), (acc_k, acc_v))
        reduce_rank(wide, scaled, slot, j, acc_l, acc_s)

    def source(i):
        away = (i + 1) // 2
        return z + flip * (2 * lax.rem(i, 2) - 1) * away

    def visit(i, j):
        zz = source(i)

        @pl.when(used(j))
        def _():
            @pl.when(i > 0)
            def _():
                pair_copy(j, zz, c).wait_recv()
                if lend:

                    @pl.when(jnp.logical_not(held(j, zz)))
                    def _():
                        each_way(j, zz, lambda copy: copy.start())

                else:
                    each_way(j, zz, lambda copy: copy.start())
                pair_copy(j, zz, c).start()
                if lend:

                    @pl.when(at_inner & (j == lent))
                    def _():
                        lend_x(zz, lambda copy: copy.start())

            add_shard(j, zz, c)

    def complete(i, j):
        zz = source(i)

        @pl.when(used(j))
        def _():
            pair_copy(j, zz, 1 - c).wait_recv()
            add_shard(j, zz, 1 - c)

    def normed(acc_rank, acc_square, rows):
        inv_rms = lax.rsqrt(jnp.sum(acc_square[rows], axis=1, keepdims=True) / model + 1e-06)
        return acc_rank[rows] * inv_rms, inv_rms

    def faded(low_rank, gate_up, gate_bias, start):
        gate = gate_bias[...] + jnp.dot(
            jnp.concatenate(split3(low_rank), axis=1),
            jnp.concatenate([gate_up[...]] * 3, axis=0),
            preferred_element_type=F32,
        )
        log_decay = (jnp.minimum(gate, 0.0) - jnp.log1p(jnp.exp(-jnp.abs(gate)))) / 16.0
        later = (
            lax.broadcasted_iota(jnp.int32, (CHUNK, CHUNK), 1)
            > lax.broadcasted_iota(jnp.int32, (CHUNK, CHUNK), 0)
        ).astype(BF16)
        suffix = start + jnp.dot(
            jnp.concatenate([later] * 3, axis=1),
            jnp.concatenate(split3(log_decay), axis=0),
            preferred_element_type=F32,
        )
        return jnp.exp(suffix), start + jnp.sum(log_decay, axis=0, keepdims=True)

    def fade_chunk(j, low_rank, inv_rms):
        weights, total = faded(low_rank, up, bias, carry[...])
        fade[...] = weights
        scale[...] = jnp.broadcast_to(inv_rms, scale.shape)
        carry[...] = total

        @pl.when(lax.rem(j, per_seq) == per_seq - 1)
        def _():
            send_total(j // per_seq)

    def finish_chunk(j):
        seq = j // per_seq

        @pl.when(lax.rem(j, per_seq) == 0)
        def _():
            carry[...] = jnp.zeros_like(carry)
            state[seq] = jnp.zeros(state.shape[1:], F32)

        last = lax.rem(j, per_seq) == per_seq - 1

        @pl.when(used(j))
        def _():
            known = at_end & (j == tail) if lend else j < 0

            @pl.when(jnp.logical_not(known))
            def _():
                fade_chunk(j, *normed(acc_l, acc_s, j))

            inv_rms = scale[:, :1]
            keys = (acc_k[j] * inv_rms).astype(BF16).astype(F32)
            weighted = keys * fade[...]
            values = (acc_v[j] * inv_rms).astype(BF16)
            for h in range(heads):
                part = weighted[:, h * DK : (h + 1) * DK].T.astype(BF16)
                rows = pl.ds(h * DK, DK)
                state[seq, rows, :] = state[seq, rows, :] + jnp.dot(
                    part, values[:, h * DV : (h + 1) * DV], preferred_element_type=F32
                )

        if lend:

            @pl.when(jnp.logical_not(used(j)))
            def _():
                send_total(seq)

        @pl.when(last)
        def _():
            send_terms(seq)

    def tot_copy(seq, peer, slot):
        return pltpu.make_async_remote_copy(
            src_ref=tots.at[seq, sp],
            dst_ref=tots.at[seq, slot],
            send_sem=tot_send.at[seq, peer],
            recv_sem=tot_recv.at[seq, slot],
            device_id={"sp": peer},
            device_id_type=MESH,
        )

    def term_copy(seq, peer, slot):
        return pltpu.make_async_remote_copy(
            src_ref=terms.at[seq, peer],
            dst_ref=landed.at[seq, slot],
            send_sem=term_send.at[seq, peer],
            recv_sem=term_recv.at[seq, slot],
            device_id={"sp": peer},
            device_id_type=MESH,
        )

    def read_copy(seq, peer, slot):
        return pltpu.make_async_remote_copy(
            src_ref=reads.at[seq, sp],
            dst_ref=reads.at[seq, slot],
            send_sem=read_send.at[seq, peer],
            recv_sem=read_recv.at[seq, slot],
            device_id={"sp": peer},
            device_id_type=MESH,
        )

    def send_total(seq):
        tots[seq, sp] = carry[...]
        for peer in peers:
            tot_copy(seq, peer, sp).start()

    def send_terms(seq):
        for h in range(heads):
            for p in range(n_sp):
                row = h * DK + p * share
                terms[seq, p, h] = state[seq, row : row + share, :].astype(BF16)
        for peer in peers:
            term_copy(seq, peer, sp).start()

    def await_back(n):
        both = (back_tots, back_terms)[n]
        for head in range(heads):
            for core in range(2):
                lines = pl.ds(2 * core, 2)
                pltpu.make_async_remote_copy(
                    src_ref=both.at[head, lines],
                    dst_ref=both.at[head, lines],
                    send_sem=back_send.at[n, 0],
                    recv_sem=back_recv.at[n, head, core],
                    device_id={"tp": inner * 2 + c},
                    device_id_type=MESH,
                ).wait_recv()

    def column(row, begin, size):
        chosen = (
            lax.broadcasted_iota(jnp.int32, (size, DK), 0) + begin
            == lax.broadcasted_iota(jnp.int32, (size, DK), 1)
        )
        return jnp.sum(jnp.where(chosen, row, 0.0), axis=1, keepdims=True)

    def query(seq, h):
        return query_ref[seq : seq + 1, h * DK : (h + 1) * DK].astype(F32)

    def send_parts(seq):
        for peer in peers:
            tot_copy(seq, peer, peer).wait_recv()
        for h in range(heads):
            after = jnp.zeros((1, DK), F32)
            for p in range(n_sp):
                total = tots[seq, p][:, h * DK : (h + 1) * DK]
                after = after + jnp.where(p > sp, total, 0.0)
            asked = column(query(seq, h) * jnp.exp(after), 0, DK)
            reads[seq, sp, h : h + 1, :] = jnp.sum(
                asked * state[seq, h * DK : (h + 1) * DK, :], axis=0, keepdims=True
            )
        for peer in peers:
            read_copy(seq, peer, sp).start()

    def sum_terms(seq, loaned):
        if loaned:
            pl.when(at_end)(lambda: await_back(0))
        after = [jnp.zeros((1, DK), F32)] * heads
        factors = [None] * n_sp
        back_factors = [None] * n_sp
        for p in reversed(range(n_sp)):
            factors[p] = [column(jnp.exp(row), sp * share, share) for row in after]
            after = [after[h] + tots[seq, p][:, h * DK : (h + 1) * DK] for h in range(heads)]
            if loaned:
                back_factors[p] = [column(jnp.exp(row), sp * share, share) for row in after]
                after = [after[h] + back_tots[h, p] for h in range(heads)]
        for peer in peers:
            term_copy(seq, peer, peer).wait_recv()
        if loaned:
            pl.when(at_end)(lambda: await_back(1))
        for h in range(heads):
            own = state[seq, pl.ds(pl.multiple_of(h * DK + sp * share, share), share), :]
            total = jnp.zeros((share, DV), F32)
            for p in range(n_sp):
                block = jnp.where(p == sp, own, landed[seq, p, h].astype(F32))
                total = total + factors[p][h] * block
                if loaned:
                    total = total + back_factors[p][h] * back_terms[h, p].astype(F32)
            cache_ref[seq, h] = total.astype(BF16)

    def send_reads(seq):
        for peer in peers:
            tot_copy(seq, peer, peer).wait_recv()
        sum_terms(seq, True)
        for h in range(heads):
            reads[seq, sp, h : h + 1, :] = jnp.sum(
                column(query(seq, h), sp * share, share) * cache_ref[seq, h].astype(F32),
                axis=0,
                keepdims=True,
            )
        for peer in peers:
            read_copy(seq, peer, sp).start()

    def give_read(seq):
        for peer in peers:
            read_copy(seq, peer, peer).wait_recv()
        parts_ref[seq] = reads[seq]

    def lent_scaled(slot):
        wide = lent_x[:, slot // 2, lax.rem(slot, 2)].reshape(2 * CHUNK, feats).astype(F32)
        return wide, (wide * gain_ref[slot]).astype(BF16)

    def work_off():
        every = slice(None)

        def collect(slot, _):
            zz, cc = slot // 2, lax.rem(slot, 2)
            for line in range(2):
                mine = 2 * c + line == sp

                @pl.when(mine)
                def _():
                    lent_x[line, zz, cc] = xbuf[lent, zz, cc]

                @pl.when(jnp.logical_not(mine))
                def _():
                    pltpu.make_async_remote_copy(
                        src_ref=lent_x.at[line, zz, cc],
                        dst_ref=lent_x.at[line, zz, cc],
                        send_sem=lent_x_send.at[zz, 0],
                        recv_sem=lent_x_recv.at[line, zz, cc],
                        device_id={"tp": tp + 1 - 2 * c},
                        device_id_type=MESH,
                    ).wait_recv()

            wide, scaled = lent_scaled(slot)
            reduce_rank(wide, scaled, slot, every, lent_l, lent_s)
            return 0

        lax.fori_loop(0, slots, collect, 0)
        blocks = [slice(line * CHUNK, (line + 1) * CHUNK) for line in range(2)]
        for line, rows in enumerate(blocks):
            low_rank, inv_rms = normed(lent_l, lent_s, rows)
            weights, total = faded(low_rank, lent_up, lent_bias, jnp.zeros((1, DK), F32))
            lent_fade[rows] = weights
            lent_scale[rows] = jnp.broadcast_to(inv_rms, weights.shape)
            lent_tots[line] = total
        for p in range(n_sp):
            give_back(0, p).start()

        def multiply(slot, _):
            pair_w(slot, lambda copy: copy.wait_recv())

            @pl.when(c == sp // 2)
            def _():
                pair_w(slot, lambda copy: copy.start())

            _, scaled = lent_scaled(slot)
            project(scaled, slot, every, (lent_wk, lent_wv), (lent_k, lent_v))
            return 0

        lax.fori_loop(0, slots, multiply, 0)
        for line, rows in enumerate(blocks):
            inv_rms = lent_scale[rows, :1]
            keys = (lent_k[rows] * inv_rms).astype(BF16).astype(F32)
            weighted = keys * lent_fade[rows]
            values = (lent_v[rows] * inv_rms).astype(BF16)
            block = jnp.dot(weighted.T.astype(BF16), values, preferred_element_type=F32)
            for p in range(n_sp):
                lent_terms[p, line] = block[p * share : (p + 1) * share].astype(BF16)
        for p in range(n_sp):
            give_back(1, p).start()

    def send_hint():
        low_rank, inv_rms = normed(acc_l, acc_s, tail)
        spread = jnp.broadcast_to(inv_rms, (CHUNK, 128 - low_rank.shape[1]))
        hint[...] = jnp.concatenate([low_rank, spread], axis=1).T[: hint.shape[0]]
        hint_copy().start()

        def release(i, _):
            zz = source(i)

            @pl.when((zz >= 0) & (zz < n_z) & held(tail, zz))
            def _():
                each_way(tail, zz, lambda copy: copy.start())

            return 0

        lax.fori_loop(1, final_step + 1, release, 0)

    def take_hint():
        hint_copy().wait_recv()
        rank = wd.shape[0]
        full = jnp.concatenate(
            [hint[...], jnp.zeros((128 - hint.shape[0], CHUNK), F32)], axis=0
        ).T
        fade_chunk(tail, full[:, :rank], full[:, rank : rank + 1])

        overdue(visit)

    def overdue(act):
        def one(i, _):
            zz = source(i)

            @pl.when((zz >= 0) & (zz < n_z))
            def _():
                act(i, tail)

            return 0

        lax.fori_loop(2, final_step, one, 0)

    steps = 2 * n_z - 2

    def ready(i, j):
        zz = source(i)
        inside = (zz >= 0) & (zz < n_z)
        if lend:
            inside = inside & jnp.logical_not(at_end & (j == tail) & (i > 1) & (i < final_step))
        return inside

    def settle(i, j):
        final = i == final_step
        closing = final & (j == tail)

        @pl.when(ready(i, j))
        def _():
            if lend:
                pl.when(at_end & closing)(lambda: overdue(complete))
            complete(i, j)
            if lend:
                pl.when(at_inner & closing)(send_hint)

            @pl.when(final)
            def _():
                finish_chunk(j)

    def step(t, _):
        i, j = t // chunks, lax.rem(t, chunks)
        last_i, last_j = (t - 1) // chunks, lax.rem(t - 1, chunks)
        early = at_end & (i == final_step) & (j == tail) if lend else t < 0
        if lend:

            @pl.when(early)
            def _():
                settle(last_i, last_j)
                take_hint()

            @pl.when(lender & (t == 2 * chunks))
            def _():
                def lend_slot(slot, _):
                    lend_w(slot, lambda copy: copy.start())
                    return 0

                lax.fori_loop(0, slots, lend_slot, 0)

        @pl.when(ready(i, j))
        def _():
            visit(i, j)

        @pl.when(jnp.logical_not(early))
        def _():
            settle(last_i, last_j)

        return 0

    visit(0, 0)
    lax.fori_loop(1, steps * chunks, step, 0)
    settle(steps - 1, chunks - 1)
    if lend:

        @pl.when(at_inner)
        def _():
            send_reads(LENT_SEQ)
            work_off()

    rest = [seq for seq in range(seqs) if not (lend and seq == LENT_SEQ)]
    for seq in rest:
        send_parts(seq)
    if lend:
        pl.when(jnp.logical_not(at_inner))(lambda: send_reads(LENT_SEQ))
    for seq in rest:
        sum_terms(seq, False)

    def drain(i, _):
        zz = source(i)

        @pl.when((zz >= 0) & (zz < n_z))
        def _():
            def inside(j, _):
                @pl.when((i == 0) | used(j))
                def _():
                    each_way(j, zz, lambda copy: copy.wait_send())

                @pl.when(used(j))
                def _():
                    pair_copy(j, zz, c).wait_send()

                return 0

            lax.fori_loop(0, chunks, inside, 0)

        return 0

    lax.fori_loop(0, 2 * n_z - 2, drain, 0)
    if lend:

        def drain_slot(slot, _):
            pl.when(lender)(lambda: lend_w(slot, lambda copy: copy.wait_send()))

            @pl.when(at_inner & (c == sp // 2))
            def _():
                pair_w(slot, lambda copy: copy.wait_send())

            return 0

        lax.fori_loop(0, slots, drain_slot, 0)

        @pl.when(at_inner)
        def _():
            for zz in range(n_z):
                lend_x(zz, lambda copy: copy.wait_send())
            for p in range(n_sp):
                give_back(0, p).wait_send()
                give_back(1, p).wait_send()
            hint_copy().wait_send()

    for seq in range(seqs):
        give_read(seq)
    for seq in range(seqs):
        for peer in peers:
            tot_copy(seq, peer, sp).wait_send()
            term_copy(seq, peer, sp).wait_send()
            read_copy(seq, peer, sp).wait_send()


def norm_kernel(cache_in, parts_ref, gain_ref, cache_ref, read_ref):
    cache_ref[...] = cache_in[...]
    seqs, n_sp, heads, _ = parts_ref.shape
    for seq in range(seqs):
        readout = parts_ref[seq, 0]
        for p in range(1, n_sp):
            readout = readout + parts_ref[seq, p]
        mean = jnp.mean(readout * readout, axis=-1, keepdims=True)
        normed = (readout * lax.rsqrt(mean + 1e-06) * gain_ref[...]).astype(BF16)
        for h in range(heads):
            read_ref[seq : seq + 1, h * DV : (h + 1) * DV] = normed[h : h + 1, :]


def per_device(
    n_sp,
    n_z,
    inputs,
    in_gain,
    key_weight,
    value_weight,
    decay_down,
    decay_up,
    decay_bias,
    new_query,
    out_gain,
):
    seqs, span, feats = inputs.shape
    model, key_cols = key_weight.shape
    value_cols = value_weight.shape[1]
    rank = decay_down.shape[1]
    heads = key_cols // DK
    chunks = seqs * (span // CHUNK)
    share = DK // n_sp
    slots = 2 * n_z
    vmem = pl.BlockSpec(memory_space=pltpu.VMEM)
    hbm = pl.BlockSpec(memory_space=pl.ANY)
    dma = pltpu.SemaphoreType.DMA
    lent = []
    if lends(n_sp, n_z, heads):
        lent = [
            pltpu.VMEM((2, n_z, 2, CHUNK, feats), BF16),
            pltpu.VMEM((model, DK), BF16),
            pltpu.VMEM((model, DV), BF16),
            pltpu.VMEM((rank, DK), BF16),
            pltpu.VMEM((1, DK), F32),
            pltpu.VMEM((2 * CHUNK, DK), F32),
            pltpu.VMEM((2 * CHUNK, DV), F32),
            pltpu.VMEM((2 * CHUNK, rank), F32),
            pltpu.VMEM((2 * CHUNK, 128), F32),
            pltpu.VMEM((2 * CHUNK, DK), F32),
            pltpu.VMEM((2 * CHUNK, DK), F32),
            pltpu.VMEM((rank + 8, CHUNK), F32),
            pltpu.VMEM((n_sp, 2, share, DV), BF16),
            pltpu.VMEM((2, 1, DK), F32),
            pltpu.VMEM((heads, n_sp, share, DV), BF16),
            pltpu.VMEM((heads, n_sp, 1, DK), F32),
            dma,
            dma,
            dma((n_z, n_sp - 1)),
            dma((2, n_z, 2)),
            dma((2, slots)),
            dma((2, slots)),
            dma((2, slots)),
            dma((2, n_sp)),
            dma((2, heads, 2)),
        ]
    cache, parts = pl.pallas_call(
        functools.partial(kernel, n_sp, n_z),
        out_shape=(
            jax.ShapeDtypeStruct((seqs, heads, share, DV), BF16),
            jax.ShapeDtypeStruct((seqs, n_sp, heads, DV), F32),
        ),
        in_specs=[hbm] * 8,
        out_specs=(vmem, vmem),
        scratch_shapes=[
            pltpu.VMEM((chunks, n_z, 2, CHUNK, feats), BF16),
            pltpu.VMEM((model, key_cols), BF16),
            pltpu.VMEM((model, value_cols), BF16),
            pltpu.VMEM((rank, model), BF16),
            pltpu.VMEM((rank, key_cols), BF16),
            pltpu.VMEM((1, key_cols), F32),
            pltpu.VMEM((slots, 1, feats), F32),
            pltpu.VMEM((seqs, key_cols), BF16),
            pltpu.VMEM((chunks, CHUNK, key_cols), F32),
            pltpu.VMEM((chunks, CHUNK, value_cols), F32),
            pltpu.VMEM((chunks, CHUNK, rank), F32),
            pltpu.VMEM((chunks, CHUNK, 128), F32),
            pltpu.VMEM((seqs, key_cols, DV), F32),
            pltpu.VMEM((1, key_cols), F32),
            pltpu.VMEM((CHUNK, key_cols), F32),
            pltpu.VMEM((CHUNK, 128), F32),
            pltpu.VMEM((seqs, n_sp, 1, key_cols), F32),
            pltpu.VMEM((seqs, n_sp, heads, share, DV), BF16),
            pltpu.VMEM((seqs, n_sp, heads, share, DV), BF16),
            pltpu.VMEM((seqs, n_sp, heads, DV), F32),
            dma((11,)),
            dma((chunks,)),
            dma((chunks, n_z, 2)),
            dma((chunks, n_z)),
            dma((chunks, n_z, 2)),
            dma((seqs, n_sp)),
            dma((seqs, n_sp)),
            dma((seqs, n_sp)),
            dma((seqs, n_sp)),
            dma((seqs, n_sp)),
            dma((seqs, n_sp)),
        ]
        + lent,
        compiler_params=pltpu.CompilerParams(
            collective_id=0, has_side_effects=True, vmem_limit_bytes=60 * 1024 * 1024
        ),
    )(
        inputs,
        in_gain.reshape(slots, 1, feats),
        key_weight,
        value_weight,
        decay_down.T,
        decay_up,
        decay_bias.reshape(1, -1),
        new_query,
    )
    return pl.pallas_call(
        norm_kernel,
        out_shape=(
            jax.ShapeDtypeStruct((seqs, heads, share, DV), BF16),
            jax.ShapeDtypeStruct((seqs, heads * DV), BF16),
        ),
        in_specs=[vmem, vmem, vmem],
        out_specs=(vmem, vmem),
    )(cache, parts, out_gain.reshape(1, -1))


def solution(mesh):
    in_specs = (
        P(None, "sp", "tp"),
        P(),
        P(None, "tp"),
        P(None, "tp"),
        P(),
        P(),
        P(),
        P(None, "tp"),
        P(),
    )
    out_specs = (P(None, "tp", "sp", None), P(None, "tp"))
    return jax.shard_map(
        functools.partial(per_device, mesh.shape["sp"], mesh.shape["tp"] // 2),
        mesh=mesh,
        in_specs=in_specs,
        out_specs=out_specs,
        check_vma=False,
    )
```

```python
import functools

import jax
import jax.numpy as jnp
from jax import lax
from jax.experimental import pallas as pl
from jax.experimental.pallas import tpu as pltpu
from jax.sharding import PartitionSpec as P

DK = 128
DV = 256
CHUNK = 128
LENT_SEQ = 0
MESH = pl.DeviceIdType.MESH
F32 = jnp.float32
BF16 = jnp.bfloat16


def split3(value):
    high = value.astype(BF16)
    rest = value - high.astype(F32)
    middle = rest.astype(BF16)
    low = (rest - middle.astype(F32)).astype(BF16)
    return high, middle, low


def lends(n_sp, n_z, heads):
    return n_z >= 4 and n_sp == 2 * heads


def kernel(
    n_sp,
    n_z,
    x_ref,
    gain_hbm,
    wk_hbm,
    wv_hbm,
    wd_hbm,
    up_hbm,
    bias_hbm,
    query_hbm,
    cache_ref,
    parts_ref,
    xbuf,
    wk,
    wv,
    wd,
    up,
    bias,
    gain_ref,
    query_ref,
    acc_k,
    acc_v,
    acc_l,
    acc_s,
    state,
    carry,
    fade,
    scale,
    tots,
    terms,
    landed,
    reads,
    load_sem,
    own_sem,
    hop_send,
    pair_send,
    recv,
    tot_send,
    tot_recv,
    term_send,
    term_recv,
    read_send,
    read_recv,
    lent_x=None,
    lent_w=None,
    lent_up=None,
    lent_bias=None,
    lent_kv=None,
    lent_l=None,
    lent_s=None,
    lent_fade=None,
    lent_scale=None,
    hint=None,
    lent_terms=None,
    sent_tots=None,
    back_terms=None,
    back_tots=None,
    hint_send=None,
    hint_recv=None,
    lent_x_send=None,
    lent_x_recv=None,
    lent_w_send=None,
    lent_w_pair=None,
    lent_w_recv=None,
    back_send=None,
    back_recv=None,
):
    seqs, span, feats = x_ref.shape
    per_seq = span // CHUNK
    chunks = seqs * per_seq
    heads = wk_hbm.shape[1] // DK
    share = DK // n_sp
    slots = 2 * n_z
    model = slots * feats
    lend = lends(n_sp, n_z, heads)
    lent = LENT_SEQ * per_seq + per_seq - 1
    tail = chunks - 1
    relayed = min(slots, chunks // 2 + 1)
    sp = lax.axis_index("sp")
    tp = lax.axis_index("tp")
    z = tp // 2
    c = lax.rem(tp, 2)
    key_cols = heads * DK
    at_end = (z == 0) | (z == n_z - 1)
    low_half = z < n_z // 2
    end = jnp.where(low_half, 0, n_z - 1)
    inner = jnp.where(low_half, 1, n_z - 2)
    at_inner = z == inner
    flip = jnp.where(low_half, 1, -1)
    reach = jnp.where(low_half, n_z - 1 - z, z)
    final_step = 2 * reach - 1
    lender = at_end & (c == sp // 2)
    peers = [lax.rem(sp + off, n_sp) for off in range(1, n_sp)]

    first = pl.multiple_of(tp * key_cols, key_cols)
    loads = [
        pltpu.make_async_copy(wk_hbm, wk, load_sem.at[0]),
        pltpu.make_async_copy(wv_hbm, wv, load_sem.at[1]),
        pltpu.make_async_copy(wd_hbm, wd, load_sem.at[2]),
        pltpu.make_async_copy(up_hbm.at[:, pl.ds(first, key_cols)], up, load_sem.at[3]),
        pltpu.make_async_copy(bias_hbm.at[:, pl.ds(first, key_cols)], bias, load_sem.at[4]),
        pltpu.make_async_copy(gain_hbm, gain_ref, load_sem.at[5]),
        pltpu.make_async_copy(query_hbm, query_ref, load_sem.at[6]),
    ]
    if lend:
        other = pl.multiple_of((end * 2 * heads + sp) * DK, DK)
        loads += [
            pltpu.make_async_copy(up_hbm.at[:, pl.ds(other, DK)], lent_up, load_sem.at[7]),
            pltpu.make_async_copy(bias_hbm.at[:, pl.ds(other, DK)], lent_bias, load_sem.at[8]),
        ]

    def stage_w(act):
        head = lax.rem(sp, 2)
        for n, (src, width, begin) in enumerate(((wk_hbm, DK, 0), (wv_hbm, DV, DK))):
            columns = pl.ds(pl.multiple_of(head * width, width), width)
            dst = lent_w.at[:, begin : begin + width]
            act(pltpu.make_async_copy(src.at[:, columns], dst, load_sem.at[9 + n]))

    def piece(j, zz, cc):
        return (j * n_z + zz) * 2 + cc

    def chunk_rows(j):
        seq = j // per_seq
        start = (per_seq - 1 - lax.rem(j, per_seq)) * CHUNK
        return seq, pl.multiple_of(start, CHUNK)

    def own_copy(j):
        seq, start = chunk_rows(j)
        return pltpu.make_async_copy(
            x_ref.at[seq, pl.ds(start, CHUNK), :], xbuf.at[piece(j, z, c)], own_sem.at[j]
        )

    def hop_copy(j, zz, way):
        return pltpu.make_async_remote_copy(
            src_ref=xbuf.at[piece(j, zz, c)],
            dst_ref=xbuf.at[piece(j, zz, c)],
            send_sem=hop_send,
            recv_sem=recv.at[j, zz, c],
            device_id={"tp": (z + 2 * way - 1) * 2 + c},
            device_id_type=MESH,
        )

    def pair_copy(j, zz, cc):
        return pltpu.make_async_remote_copy(
            src_ref=xbuf.at[piece(j, zz, cc)],
            dst_ref=xbuf.at[piece(j, zz, cc)],
            send_sem=pair_send,
            recv_sem=recv.at[j, zz, cc],
            device_id={"tp": tp + 1 - 2 * c},
            device_id_type=MESH,
        )

    def each_way(j, zz, act):
        for way, edge in ((0, 0), (1, n_z - 1)):
            there = z + 2 * way - 1
            beyond = (zz >= z) if way == 0 else (zz <= z)
            wanted = (z != edge) & beyond
            if lend:
                wanted = wanted & ((j != lent) | (there != edge))

            @pl.when(wanted)
            def _():
                act(hop_copy(j, zz, way))

    def held(j, zz):
        return at_inner & (j == tail) & (flip * (zz - z) > 0)

    def used(j):
        if not lend:
            return j >= 0
        return (j != lent) | jnp.logical_not(at_end)

    def lend_x(zz, act):
        for peer in peers:
            act(
                pltpu.make_async_remote_copy(
                    src_ref=xbuf.at[piece(lent, zz, c)],
                    dst_ref=lent_x.at[lax.rem(sp, 2), zz, c],
                    send_sem=lent_x_send,
                    recv_sem=lent_x_recv.at[lax.rem(sp, 2)],
                    device_id={"sp": peer, "tp": z * 2 + sp // 2},
                    device_id_type=MESH,
                )
            )

    def w_copy(slot, device, send_sem):
        rows = pl.ds(pl.multiple_of(slot * feats, feats), feats)
        return pltpu.make_async_remote_copy(
            src_ref=lent_w.at[rows],
            dst_ref=lent_w.at[rows],
            send_sem=send_sem,
            recv_sem=lent_w_recv.at[slot],
            device_id={"tp": device},
            device_id_type=MESH,
        )

    def lend_w(slot):
        return w_copy(slot, inner * 2 + c, lent_w_send)

    def pair_w(slot):
        return w_copy(slot, tp + 1 - 2 * c, lent_w_pair)

    def w_copy_all(send_sem):
        return pltpu.make_async_remote_copy(
            src_ref=lent_w,
            dst_ref=lent_w,
            send_sem=send_sem,
            recv_sem=lent_w_recv.at[0],
            device_id={"tp": tp + 1 - 2 * c},
            device_id_type=MESH,
        )

    def given(n):
        both = (sent_tots, lent_terms)[n]
        return pltpu.make_async_remote_copy(
            src_ref=both,
            dst_ref=both,
            send_sem=back_send.at[n],
            recv_sem=back_recv.at[n],
            device_id={"tp": tp + 1 - 2 * c},
            device_id_type=MESH,
        )

    def hint_copy():
        return pltpu.make_async_remote_copy(
            src_ref=hint,
            dst_ref=hint,
            send_sem=hint_send,
            recv_sem=hint_recv,
            device_id={"tp": end * 2 + c},
            device_id_type=MESH,
        )

    def give_back(n, p):
        lines = pl.ds(2 * c, 2)
        src, dst = ((sent_tots.at[p], back_tots), (lent_terms.at[p], back_terms))[n]
        return pltpu.make_async_remote_copy(
            src_ref=src,
            dst_ref=dst.at[lax.rem(sp, 2), lines],
            send_sem=back_send.at[n],
            recv_sem=back_recv.at[n],
            device_id={"sp": p, "tp": end * 2 + sp // 2},
            device_id_type=MESH,
        )

    for j in range(chunks):
        own_copy(j).start()
    for load in loads:
        load.start()
    if lend:
        pl.when(lender)(lambda: stage_w(lambda copy: copy.start()))

    barrier = pltpu.get_barrier_semaphore()

    def greet(ahead, device):
        @pl.when(ahead)
        def _():
            pl.semaphore_signal(barrier, inc=1, device_id=device, device_id_type=MESH)

    close = at_end | at_inner if lend else False
    apart = jnp.logical_not(close)
    for way, edge in ((0, 0), (1, n_z - 1)):
        there = z + 2 * way - 1
        met = z != edge
        if lend:
            met = met & jnp.logical_not(close & ((there == end) | (there == inner)))
        greet(met, {"tp": there * 2 + c})
    if lend:
        for p in range(n_sp):
            for plane in (end, inner):
                for core in range(2):
                    known = close & ((p != sp) | (plane != z) | (core != c))
                    greet(known, {"sp": p, "tp": plane * 2 + core})
        greet(apart, {"tp": tp + 1 - 2 * c})
        for peer in peers:
            greet(apart, {"sp": peer})
        far = jnp.where(close, 4 * n_sp - 1 + jnp.where(at_inner, 1, 0), 2 + n_sp)
    else:
        greet(tp >= 0, {"tp": tp + 1 - 2 * c})
        for peer in peers:
            greet(tp >= 0, {"sp": peer})
        far = n_sp + jnp.where(z > 0, 1, 0) + jnp.where(z < n_z - 1, 1, 0)

    acc_k[...] = jnp.zeros_like(acc_k)
    acc_v[...] = jnp.zeros_like(acc_v)
    acc_l[...] = jnp.zeros_like(acc_l)
    acc_s[...] = jnp.zeros_like(acc_s)
    if lend:

        @pl.when(at_inner)
        def _():
            lent_kv[...] = jnp.zeros_like(lent_kv)
            lent_l[...] = jnp.zeros_like(lent_l)
            lent_s[...] = jnp.zeros_like(lent_s)

        @pl.when(jnp.logical_not(at_end))
        def _():
            back_terms[...] = jnp.zeros_like(back_terms)
            back_tots[...] = jnp.zeros_like(back_tots)

    pl.semaphore_wait(barrier, far)

    def open_chunk(j, _):
        own_copy(j).wait()
        each_way(j, z, lambda copy: copy.start())

        @pl.when(used(j))
        def _():
            pair_copy(j, z, c).start()

        return 0

    lax.fori_loop(0, chunks, open_chunk, 0)
    if lend:

        @pl.when(at_inner)
        def _():
            lend_x(z, lambda copy: copy.start())

    for load in loads:
        load.wait()
    if lend:
        pl.when(lender)(lambda: stage_w(lambda copy: copy.wait()))

    def project(scaled, slot, rows, weights, accs):
        deep = pl.ds(pl.multiple_of(slot * feats, feats), feats)
        for weight, acc in zip(weights, accs):
            acc[rows] += jnp.dot(scaled, weight[deep, :], preferred_element_type=F32)

    def reduce_rank(wide, scaled, slot, rows, acc_rank, acc_square):
        deep = pl.ds(pl.multiple_of(slot * feats, feats), feats)
        acc_rank[rows] += lax.dot_general(
            scaled, wd[:, deep], (((1,), (1,)), ((), ())), preferred_element_type=F32
        )
        square = wide * wide
        total = square[:, 0:128]
        for lane in range(128, feats, 128):
            total = total + square[:, lane : lane + 128]
        acc_square[rows] += total

    def add_shard(j, zz, cc):
        slot = zz * 2 + cc
        wide = xbuf[piece(j, zz, cc)].astype(F32)
        scaled = (wide * gain_ref[slot]).astype(BF16)
        project(scaled, slot, j, (wk, wv), (acc_k, acc_v))
        reduce_rank(wide, scaled, slot, j, acc_l, acc_s)

    def source(i):
        away = (i + 1) // 2
        return z + flip * (2 * lax.rem(i, 2) - 1) * away

    def visit(i, j):
        zz = source(i)

        @pl.when(used(j))
        def _():
            @pl.when(i > 0)
            def _():
                pair_copy(j, zz, c).wait_recv()
                if lend:

                    @pl.when(jnp.logical_not(held(j, zz)))
                    def _():
                        each_way(j, zz, lambda copy: copy.start())

                else:
                    each_way(j, zz, lambda copy: copy.start())
                pair_copy(j, zz, c).start()
                if lend:

                    @pl.when(at_inner & (j == lent))
                    def _():
                        lend_x(zz, lambda copy: copy.start())

            add_shard(j, zz, c)

    def complete(i, j):
        zz = source(i)

        @pl.when(used(j))
        def _():
            pair_copy(j, zz, 1 - c).wait_recv()
            add_shard(j, zz, 1 - c)

    def normed(acc_rank, acc_square, rows):
        inv_rms = lax.rsqrt(jnp.sum(acc_square[rows], axis=1, keepdims=True) / model + 1e-06)
        return acc_rank[rows] * inv_rms, inv_rms

    def faded(low_rank, gate_up, gate_bias, start):
        gate = gate_bias[...] + jnp.dot(
            jnp.concatenate(split3(low_rank), axis=1),
            jnp.concatenate([gate_up[...]] * 3, axis=0),
            preferred_element_type=F32,
        )
        log_decay = (jnp.minimum(gate, 0.0) - jnp.log1p(jnp.exp(-jnp.abs(gate)))) / 16.0
        later = (
            lax.broadcasted_iota(jnp.int32, (CHUNK, CHUNK), 1)
            > lax.broadcasted_iota(jnp.int32, (CHUNK, CHUNK), 0)
        ).astype(BF16)
        suffix = start + jnp.dot(
            jnp.concatenate([later] * 3, axis=1),
            jnp.concatenate(split3(log_decay), axis=0),
            preferred_element_type=F32,
        )
        return jnp.exp(suffix), start + jnp.sum(log_decay, axis=0, keepdims=True)

    def fade_chunk(j, low_rank, inv_rms):
        weights, total = faded(low_rank, up, bias, carry[...])
        fade[...] = weights
        scale[...] = jnp.broadcast_to(inv_rms, scale.shape)
        carry[...] = total

        @pl.when(lax.rem(j, per_seq) == per_seq - 1)
        def _():
            send_total(j // per_seq)

    def finish_chunk(j):
        seq = j // per_seq

        @pl.when(lax.rem(j, per_seq) == 0)
        def _():
            carry[...] = jnp.zeros_like(carry)
            state[seq] = jnp.zeros(state.shape[1:], F32)

        last = lax.rem(j, per_seq) == per_seq - 1

        @pl.when(used(j))
        def _():
            known = at_end & (j == tail) if lend else j < 0

            @pl.when(jnp.logical_not(known))
            def _():
                fade_chunk(j, *normed(acc_l, acc_s, j))

            inv_rms = scale[:, :1]
            keys = (acc_k[j] * inv_rms).astype(BF16).astype(F32)
            weighted = keys * fade[...]
            values = (acc_v[j] * inv_rms).astype(BF16)
            for h in range(heads):
                part = weighted[:, h * DK : (h + 1) * DK].T.astype(BF16)
                rows = pl.ds(h * DK, DK)
                state[seq, rows, :] = state[seq, rows, :] + jnp.dot(
                    part, values[:, h * DV : (h + 1) * DV], preferred_element_type=F32
                )

        if lend:

            @pl.when(jnp.logical_not(used(j)))
            def _():
                send_total(seq)

        @pl.when(last)
        def _():
            send_terms(seq)

    def tot_copy(seq, peer):
        return pltpu.make_async_remote_copy(
            src_ref=tots.at[seq, sp],
            dst_ref=tots.at[seq, sp],
            send_sem=tot_send.at[seq],
            recv_sem=tot_recv.at[seq],
            device_id={"sp": peer},
            device_id_type=MESH,
        )

    def term_copy(seq, peer):
        return pltpu.make_async_remote_copy(
            src_ref=terms.at[seq, peer],
            dst_ref=landed.at[seq, sp],
            send_sem=term_send.at[seq],
            recv_sem=term_recv.at[seq],
            device_id={"sp": peer},
            device_id_type=MESH,
        )

    def read_copy(seq, peer):
        return pltpu.make_async_remote_copy(
            src_ref=reads.at[seq, sp],
            dst_ref=reads.at[seq, sp],
            send_sem=read_send.at[seq],
            recv_sem=read_recv.at[seq],
            device_id={"sp": peer},
            device_id_type=MESH,
        )

    def others(ref, seq, sems):
        return pltpu.make_async_remote_copy(
            src_ref=ref.at[seq, pl.ds(0, n_sp - 1)],
            dst_ref=ref.at[seq, pl.ds(0, n_sp - 1)],
            send_sem=sems[0].at[seq],
            recv_sem=sems[1].at[seq],
            device_id={"sp": peers[0]},
            device_id_type=MESH,
        )

    def all_tots(seq):
        return others(tots, seq, (tot_send, tot_recv))

    def all_terms(seq):
        return others(landed, seq, (term_send, term_recv))

    def all_reads(seq):
        return others(reads, seq, (read_send, read_recv))

    def send_total(seq):
        tots[seq, sp] = carry[...]
        for peer in peers:
            tot_copy(seq, peer).start()

    def send_terms(seq):
        for h in range(heads):
            for p in range(n_sp):
                row = h * DK + p * share
                terms[seq, p, h] = state[seq, row : row + share, :].astype(BF16)
        for peer in peers:
            term_copy(seq, peer).start()

    def back_copy(n):
        both = (back_tots, back_terms)[n]
        return pltpu.make_async_remote_copy(
            src_ref=both,
            dst_ref=both,
            send_sem=back_send.at[n],
            recv_sem=back_recv.at[n],
            device_id={"tp": inner * 2 + c},
            device_id_type=MESH,
        )

    def column(row, begin, size):
        chosen = (
            lax.broadcasted_iota(jnp.int32, (size, DK), 0) + begin
            == lax.broadcasted_iota(jnp.int32, (size, DK), 1)
        )
        return jnp.sum(jnp.where(chosen, row, 0.0), axis=1, keepdims=True)

    def query(seq, h):
        return query_ref[seq : seq + 1, h * DK : (h + 1) * DK].astype(F32)

    def send_parts(seq):
        all_tots(seq).wait_recv()
        for h in range(heads):
            after = jnp.zeros((1, DK), F32)
            for p in range(n_sp):
                total = tots[seq, p][:, h * DK : (h + 1) * DK]
                after = after + jnp.where(p > sp, total, 0.0)
            asked = column(query(seq, h) * jnp.exp(after), 0, DK)
            reads[seq, sp, h : h + 1, :] = jnp.sum(
                asked * state[seq, h * DK : (h + 1) * DK, :], axis=0, keepdims=True
            )
        for peer in peers:
            read_copy(seq, peer).start()

    def sum_terms(seq, loaned):
        if loaned:
            pl.when(at_end)(lambda: back_copy(0).wait_recv())
        after = [jnp.zeros((1, DK), F32)] * heads
        factors = [None] * n_sp
        back_factors = [None] * n_sp
        for p in reversed(range(n_sp)):
            factors[p] = [column(jnp.exp(row), sp * share, share) for row in after]
            after = [after[h] + tots[seq, p][:, h * DK : (h + 1) * DK] for h in range(heads)]
            if loaned:
                back_factors[p] = [column(jnp.exp(row), sp * share, share) for row in after]
                after = [after[h] + back_tots[h, p] for h in range(heads)]
        all_terms(seq).wait_recv()
        if loaned:
            pl.when(at_end)(lambda: back_copy(1).wait_recv())
        for h in range(heads):
            own = state[seq, pl.ds(pl.multiple_of(h * DK + sp * share, share), share), :]
            total = jnp.zeros((share, DV), F32)
            for p in range(n_sp):
                block = jnp.where(p == sp, own, landed[seq, p, h].astype(F32))
                total = total + factors[p][h] * block
                if loaned:
                    total = total + back_factors[p][h] * back_terms[h, p].astype(F32)
            cache_ref[seq, h] = total.astype(BF16)

    def send_reads(seq):
        all_tots(seq).wait_recv()
        sum_terms(seq, True)
        for h in range(heads):
            reads[seq, sp, h : h + 1, :] = jnp.sum(
                column(query(seq, h), sp * share, share) * cache_ref[seq, h].astype(F32),
                axis=0,
                keepdims=True,
            )
        for peer in peers:
            read_copy(seq, peer).start()

    def give_read(seq):
        all_reads(seq).wait_recv()
        parts_ref[seq] = reads[seq]

    def lent_scaled(slot):
        wide = lent_x[:, slot // 2, lax.rem(slot, 2)].reshape(2 * CHUNK, feats).astype(F32)
        return wide, (wide * gain_ref[slot]).astype(BF16)

    def work_off():
        every = slice(None)

        def collect(slot, _):
            zz, cc = slot // 2, lax.rem(slot, 2)
            for line in range(2):

                @pl.when(2 * c + line == sp)
                def _():
                    lent_x[line, zz, cc] = xbuf[piece(lent, zz, cc)]

            wide, scaled = lent_scaled(slot)
            reduce_rank(wide, scaled, slot, every, lent_l, lent_s)
            return 0

        for line in range(2):

            @pl.when(2 * c + line != sp)
            def _():
                pltpu.make_async_remote_copy(
                    src_ref=lent_x.at[line],
                    dst_ref=lent_x.at[line],
                    send_sem=lent_x_send,
                    recv_sem=lent_x_recv.at[line],
                    device_id={"tp": tp + 1 - 2 * c},
                    device_id_type=MESH,
                ).wait_recv()

        lax.fori_loop(0, slots, collect, 0)
        blocks = [slice(line * CHUNK, (line + 1) * CHUNK) for line in range(2)]
        for line, rows in enumerate(blocks):
            low_rank, inv_rms = normed(lent_l, lent_s, rows)
            weights, total = faded(low_rank, lent_up, lent_bias, jnp.zeros((1, DK), F32))
            lent_fade[rows] = weights
            lent_scale[rows] = jnp.broadcast_to(inv_rms, weights.shape)
            for q in range(n_sp):
                sent_tots[q, line] = total
        for p in range(n_sp):
            give_back(0, p).start()
        send_reads(LENT_SEQ)

        def multiply(slot, _):
            @pl.when((c != sp // 2) | (slot >= relayed))
            def _():
                pair_w(slot).wait_recv()

            @pl.when((c == sp // 2) & (slot >= relayed))
            def _():
                pair_w(slot).start()

            _, scaled = lent_scaled(slot)
            project(scaled, slot, every, (lent_w,), (lent_kv,))
            return 0

        lax.fori_loop(0, slots, multiply, 0)
        for line, rows in enumerate(blocks):
            inv_rms = lent_scale[rows, :1]
            keys = (lent_kv[rows, :DK] * inv_rms).astype(BF16).astype(F32)
            weighted = keys * lent_fade[rows]
            values = (lent_kv[rows, DK:] * inv_rms).astype(BF16)
            block = jnp.dot(weighted.T.astype(BF16), values, preferred_element_type=F32)
            for p in range(n_sp):
                lent_terms[p, line] = block[p * share : (p + 1) * share].astype(BF16)
        for p in range(n_sp):
            give_back(1, p).start()

    def send_hint():
        low_rank, inv_rms = normed(acc_l, acc_s, tail)
        spread = jnp.broadcast_to(inv_rms, (CHUNK, 128 - low_rank.shape[1]))
        hint[...] = jnp.concatenate([low_rank, spread], axis=1).T[: hint.shape[0]]
        hint_copy().start()

        def release(i, _):
            zz = source(i)

            @pl.when((zz >= 0) & (zz < n_z) & held(tail, zz))
            def _():
                each_way(tail, zz, lambda copy: copy.start())

            return 0

        lax.fori_loop(1, final_step + 1, release, 0)

    def take_hint():
        hint_copy().wait_recv()
        rank = wd.shape[0]
        full = jnp.concatenate(
            [hint[...], jnp.zeros((128 - hint.shape[0], CHUNK), F32)], axis=0
        ).T
        fade_chunk(tail, full[:, :rank], full[:, rank : rank + 1])

        overdue(visit)

    def overdue(act):
        def one(i, _):
            zz = source(i)

            @pl.when((zz >= 0) & (zz < n_z))
            def _():
                act(i, tail)

            return 0

        lax.fori_loop(2, final_step, one, 0)

    steps = 2 * n_z - 2

    def ready(i, j):
        zz = source(i)
        inside = (zz >= 0) & (zz < n_z)
        if lend:
            inside = inside & jnp.logical_not(at_end & (j == tail) & (i > 1) & (i < final_step))
        return inside

    def settle(i, j):
        final = i == final_step
        closing = final & (j == tail)

        @pl.when(ready(i, j))
        def _():
            if lend:
                pl.when(at_end & closing)(lambda: overdue(complete))
            complete(i, j)
            if lend:
                pl.when(at_inner & closing)(send_hint)

            @pl.when(final)
            def _():
                finish_chunk(j)

    def step(t, _):
        i, j = t // chunks, lax.rem(t, chunks)
        last_i, last_j = (t - 1) // chunks, lax.rem(t - 1, chunks)
        early = at_end & (i == final_step) & (j == tail) if lend else t < 0
        if lend:

            @pl.when(early)
            def _():
                settle(last_i, last_j)
                take_hint()

            due = (2 * j + 1) // 3
            relaying = at_inner & (c == sp // 2) & (i == final_step) & ((3 * due + 1) // 2 == j)

            @pl.when(relaying & (due < relayed))
            def _():
                pair_w(due).wait_recv()
                pair_w(due).start()

            @pl.when(lender & (t == 2 * chunks))
            def _():
                def lend_slot(slot, _):
                    lend_w(slot).start()
                    return 0

                lax.fori_loop(0, slots, lend_slot, 0)

        @pl.when(ready(i, j))
        def _():
            visit(i, j)

        @pl.when(jnp.logical_not(early))
        def _():
            settle(last_i, last_j)

        return 0

    visit(0, 0)
    lax.fori_loop(1, steps * chunks, step, 0)
    settle(steps - 1, chunks - 1)
    if lend:

        @pl.when(at_inner)
        def _():
            work_off()

    rest = [seq for seq in range(seqs) if not (lend and seq == LENT_SEQ)]
    for seq in rest:
        send_parts(seq)
    if lend:
        pl.when(jnp.logical_not(at_inner))(lambda: send_reads(LENT_SEQ))
    for seq in rest:
        sum_terms(seq, False)

    def drained(count, send_sem):
        pltpu.make_async_remote_copy(
            src_ref=xbuf.at[pl.ds(0, count)],
            dst_ref=xbuf.at[pl.ds(0, count)],
            send_sem=send_sem,
            recv_sem=recv.at[0, 0, 0],
            device_id={"tp": tp + 1 - 2 * c},
            device_id_type=MESH,
        ).wait_send()

    for plane in range(n_z):
        edge = plane in (0, n_z - 1)
        hops = (0 if plane == 0 else n_z - plane) + (0 if plane == n_z - 1 else plane + 1)
        hops = hops * chunks
        pairs = n_z * chunks
        if lend and plane in (1, n_z - 2):
            hops -= n_z - 1
        if lend and edge:
            pairs -= n_z

        @pl.when(z == plane)
        def _():
            drained(hops, hop_send)
            drained(pairs, pair_send)

    if lend:
        pl.when(lender)(lambda: w_copy_all(lent_w_send).wait_send())

        @pl.when(at_inner)
        def _():
            pl.when(c == sp // 2)(lambda: w_copy_all(lent_w_pair).wait_send())
            drained(n_z * (n_sp - 1), lent_x_send)
            given(0).wait_send()
            given(1).wait_send()
            hint_copy().wait_send()

    for seq in range(seqs):
        give_read(seq)
    for seq in range(seqs):
        for kind in (all_tots, all_terms, all_reads):
            kind(seq).wait_send()


def norm_kernel(cache_in, parts_ref, gain_ref, cache_ref, read_ref):
    cache_ref[...] = cache_in[...]
    seqs, n_sp, heads, _ = parts_ref.shape
    for seq in range(seqs):
        readout = parts_ref[seq, 0]
        for p in range(1, n_sp):
            readout = readout + parts_ref[seq, p]
        mean = jnp.mean(readout * readout, axis=-1, keepdims=True)
        normed = (readout * lax.rsqrt(mean + 1e-06) * gain_ref[...]).astype(BF16)
        for h in range(heads):
            read_ref[seq : seq + 1, h * DV : (h + 1) * DV] = normed[h : h + 1, :]


def per_device(
    n_sp,
    n_z,
    inputs,
    in_gain,
    key_weight,
    value_weight,
    decay_down,
    decay_up,
    decay_bias,
    new_query,
    out_gain,
):
    seqs, span, feats = inputs.shape
    model, key_cols = key_weight.shape
    value_cols = value_weight.shape[1]
    rank = decay_down.shape[1]
    heads = key_cols // DK
    chunks = seqs * (span // CHUNK)
    share = DK // n_sp
    slots = 2 * n_z
    vmem = pl.BlockSpec(memory_space=pltpu.VMEM)
    hbm = pl.BlockSpec(memory_space=pl.ANY)
    dma = pltpu.SemaphoreType.DMA
    lent = []
    if lends(n_sp, n_z, heads):
        lent = [
            pltpu.VMEM((2, n_z, 2, CHUNK, feats), BF16),
            pltpu.VMEM((model, DK + DV), BF16),
            pltpu.VMEM((rank, DK), BF16),
            pltpu.VMEM((1, DK), F32),
            pltpu.VMEM((2 * CHUNK, DK + DV), F32),
            pltpu.VMEM((2 * CHUNK, rank), F32),
            pltpu.VMEM((2 * CHUNK, 128), F32),
            pltpu.VMEM((2 * CHUNK, DK), F32),
            pltpu.VMEM((2 * CHUNK, DK), F32),
            pltpu.VMEM((rank + 8, CHUNK), F32),
            pltpu.VMEM((n_sp, 2, share, DV), BF16),
            pltpu.VMEM((n_sp, 2, 1, DK), F32),
            pltpu.VMEM((heads, n_sp, share, DV), BF16),
            pltpu.VMEM((heads, n_sp, 1, DK), F32),
            dma,
            dma,
            dma,
            dma((2,)),
            dma,
            dma,
            dma((slots,)),
            dma((2,)),
            dma((2,)),
        ]
    cache, parts = pl.pallas_call(
        functools.partial(kernel, n_sp, n_z),
        out_shape=(
            jax.ShapeDtypeStruct((seqs, heads, share, DV), BF16),
            jax.ShapeDtypeStruct((seqs, n_sp, heads, DV), F32),
        ),
        in_specs=[hbm] * 8,
        out_specs=(vmem, vmem),
        scratch_shapes=[
            pltpu.VMEM((chunks * slots, CHUNK, feats), BF16),
            pltpu.VMEM((model, key_cols), BF16),
            pltpu.VMEM((model, value_cols), BF16),
            pltpu.VMEM((rank, model), BF16),
            pltpu.VMEM((rank, key_cols), BF16),
            pltpu.VMEM((1, key_cols), F32),
            pltpu.VMEM((slots, 1, feats), F32),
            pltpu.VMEM((seqs, key_cols), BF16),
            pltpu.VMEM((chunks, CHUNK, key_cols), F32),
            pltpu.VMEM((chunks, CHUNK, value_cols), F32),
            pltpu.VMEM((chunks, CHUNK, rank), F32),
            pltpu.VMEM((chunks, CHUNK, 128), F32),
            pltpu.VMEM((seqs, key_cols, DV), F32),
            pltpu.VMEM((1, key_cols), F32),
            pltpu.VMEM((CHUNK, key_cols), F32),
            pltpu.VMEM((CHUNK, 128), F32),
            pltpu.VMEM((seqs, n_sp, 1, key_cols), F32),
            pltpu.VMEM((seqs, n_sp, heads, share, DV), BF16),
            pltpu.VMEM((seqs, n_sp, heads, share, DV), BF16),
            pltpu.VMEM((seqs, n_sp, heads, DV), F32),
            dma((11,)),
            dma((chunks,)),
            dma,
            dma,
            dma((chunks, n_z, 2)),
            dma((seqs,)),
            dma((seqs,)),
            dma((seqs,)),
            dma((seqs,)),
            dma((seqs,)),
            dma((seqs,)),
        ]
        + lent,
        compiler_params=pltpu.CompilerParams(
            collective_id=0, has_side_effects=True, vmem_limit_bytes=60 * 1024 * 1024
        ),
    )(
        inputs,
        in_gain.reshape(slots, 1, feats),
        key_weight,
        value_weight,
        decay_down.T,
        decay_up,
        decay_bias.reshape(1, -1),
        new_query,
    )
    return pl.pallas_call(
        norm_kernel,
        out_shape=(
            jax.ShapeDtypeStruct((seqs, heads, share, DV), BF16),
            jax.ShapeDtypeStruct((seqs, heads * DV), BF16),
        ),
        in_specs=[vmem, vmem, vmem],
        out_specs=(vmem, vmem),
    )(cache, parts, out_gain.reshape(1, -1))


def solution(mesh):
    in_specs = (
        P(None, "sp", "tp"),
        P(),
        P(None, "tp"),
        P(None, "tp"),
        P(),
        P(),
        P(),
        P(None, "tp"),
        P(),
    )
    out_specs = (P(None, "tp", "sp", None), P(None, "tp"))
    return jax.shard_map(
        functools.partial(per_device, mesh.shape["sp"], mesh.shape["tp"] // 2),
        mesh=mesh,
        in_specs=in_specs,
        out_specs=out_specs,
        check_vma=False,
    )
```

```python
import functools

import jax
import jax.numpy as jnp
from jax import lax
from jax.experimental import pallas as pl
from jax.experimental.pallas import tpu as pltpu
from jax.sharding import PartitionSpec as P

DK = 128
DV = 256
CHUNK = 128
LENT_SEQ = 0
EXTRA = 64
MESH = pl.DeviceIdType.MESH
F32 = jnp.float32
BF16 = jnp.bfloat16


def split3(value):
    high = value.astype(BF16)
    rest = value - high.astype(F32)
    middle = rest.astype(BF16)
    low = (rest - middle.astype(F32)).astype(BF16)
    return high, middle, low


def lends(n_sp, n_z, heads):
    return n_z >= 4 and n_sp == 2 * heads


def kernel(
    n_sp,
    n_z,
    x_ref,
    gain_hbm,
    wk_hbm,
    wv_hbm,
    wd_hbm,
    up_hbm,
    bias_hbm,
    query_hbm,
    cache_ref,
    parts_ref,
    xbuf,
    wk,
    wv,
    wd,
    up,
    bias,
    gain_ref,
    query_ref,
    acc_k,
    acc_v,
    acc_l,
    acc_s,
    state,
    carry,
    fade,
    scale,
    tots,
    terms,
    landed,
    reads,
    load_sem,
    own_sem,
    hop_send,
    pair_send,
    recv,
    tot_send,
    tot_recv,
    term_send,
    term_recv,
    read_send,
    read_recv,
    lent_x=None,
    lent_w=None,
    lent_up=None,
    lent_bias=None,
    lent_kv=None,
    lent_l=None,
    lent_s=None,
    lent_fade=None,
    lent_scale=None,
    hint=None,
    lent_terms=None,
    sent_tots=None,
    back_terms=None,
    back_tots=None,
    asks=None,
    asked=None,
    sent_reads=None,
    back_reads=None,
    lent_state=None,
    ask_send=None,
    ask_recv=None,
    hint_send=None,
    hint_recv=None,
    lent_x_send=None,
    lent_x_recv=None,
    lent_w_send=None,
    lent_w_pair=None,
    lent_w_recv=None,
    back_send=None,
    back_recv=None,
):
    seqs, span, feats = x_ref.shape
    per_seq = span // CHUNK
    chunks = seqs * per_seq
    heads = wk_hbm.shape[1] // DK
    share = DK // n_sp
    slots = 2 * n_z
    model = slots * feats
    lend = lends(n_sp, n_z, heads)
    lent = LENT_SEQ * per_seq + per_seq - 1
    tail = chunks - 1
    split = lent - 1
    lent_rows = CHUNK + EXTRA
    relayed = min(slots - 2, chunks // 2 + 1)
    sp = lax.axis_index("sp")
    tp = lax.axis_index("tp")
    z = tp // 2
    c = lax.rem(tp, 2)
    key_cols = heads * DK
    at_end = (z == 0) | (z == n_z - 1)
    low_half = z < n_z // 2
    end = jnp.where(low_half, 0, n_z - 1)
    inner = jnp.where(low_half, 1, n_z - 2)
    at_inner = z == inner
    far_end = n_z - 1 - end
    flip = jnp.where(low_half, 1, -1)
    reach = jnp.where(low_half, n_z - 1 - z, z)
    final_step = 2 * reach - 1
    lender = at_end & (c == sp // 2)
    peers = [lax.rem(sp + off, n_sp) for off in range(1, n_sp)]

    first = pl.multiple_of(tp * key_cols, key_cols)
    loads = [
        pltpu.make_async_copy(wk_hbm, wk, load_sem.at[0]),
        pltpu.make_async_copy(wv_hbm, wv, load_sem.at[1]),
        pltpu.make_async_copy(wd_hbm, wd, load_sem.at[2]),
        pltpu.make_async_copy(up_hbm.at[:, pl.ds(first, key_cols)], up, load_sem.at[3]),
        pltpu.make_async_copy(bias_hbm.at[:, pl.ds(first, key_cols)], bias, load_sem.at[4]),
        pltpu.make_async_copy(gain_hbm, gain_ref, load_sem.at[5]),
        pltpu.make_async_copy(query_hbm, query_ref, load_sem.at[6]),
    ]
    if lend:
        other = pl.multiple_of((end * 2 * heads + sp) * DK, DK)
        loads += [
            pltpu.make_async_copy(up_hbm.at[:, pl.ds(other, DK)], lent_up, load_sem.at[7]),
            pltpu.make_async_copy(bias_hbm.at[:, pl.ds(other, DK)], lent_bias, load_sem.at[8]),
        ]

    def stage_w(act):
        head = lax.rem(sp, 2)
        for n, (src, width, begin) in enumerate(((wk_hbm, DK, 0), (wv_hbm, DV, DK))):
            columns = pl.ds(pl.multiple_of(head * width, width), width)
            dst = lent_w.at[:, begin : begin + width]
            act(pltpu.make_async_copy(src.at[:, columns], dst, load_sem.at[9 + n]))

    def piece(j, zz, cc, skip=0):
        start = ((j * n_z + zz) * 2 + cc) * CHUNK + skip
        return pl.ds(pl.multiple_of(start, 16), CHUNK - skip)

    def opening(zz, cc):
        start = ((split * n_z + zz) * 2 + cc) * CHUNK
        return pl.ds(pl.multiple_of(start, 16), EXTRA)

    def chunk_rows(j):
        seq = j // per_seq
        start = (per_seq - 1 - lax.rem(j, per_seq)) * CHUNK
        return seq, pl.multiple_of(start, CHUNK)

    def own_copy(j):
        seq, start = chunk_rows(j)
        return pltpu.make_async_copy(
            x_ref.at[seq, pl.ds(start, CHUNK), :], xbuf.at[piece(j, z, c)], own_sem.at[j]
        )

    def hop_copy(j, zz, way, skip=0):
        return pltpu.make_async_remote_copy(
            src_ref=xbuf.at[piece(j, zz, c, skip)],
            dst_ref=xbuf.at[piece(j, zz, c, skip)],
            send_sem=hop_send,
            recv_sem=recv.at[j, zz, c],
            device_id={"tp": (z + 2 * way - 1) * 2 + c},
            device_id_type=MESH,
        )

    def pair_copy(j, zz, cc, skip=0):
        return pltpu.make_async_remote_copy(
            src_ref=xbuf.at[piece(j, zz, cc, skip)],
            dst_ref=xbuf.at[piece(j, zz, cc, skip)],
            send_sem=pair_send,
            recv_sem=recv.at[j, zz, cc],
            device_id={"tp": tp + 1 - 2 * c},
            device_id_type=MESH,
        )

    def each_pair(j, zz, cc, act):
        if not lend:
            act(pair_copy(j, zz, cc))
            return
        short = at_end & (j == split)
        pl.when(short)(lambda: act(pair_copy(j, zz, cc, EXTRA)))
        pl.when(jnp.logical_not(short))(lambda: act(pair_copy(j, zz, cc)))

    def each_way(j, zz, act):
        for way, edge in ((0, 0), (1, n_z - 1)):
            there = z + 2 * way - 1
            beyond = (zz >= z) if way == 0 else (zz <= z)
            wanted = (z != edge) & beyond
            if lend:
                short = (j == split) & (there == edge)
                pl.when(wanted & short)(lambda: act(hop_copy(j, zz, way, EXTRA)))
                wanted = wanted & jnp.logical_not(short) & ((j != lent) | (there != edge))
            pl.when(wanted)(lambda: act(hop_copy(j, zz, way)))

    def held(j, zz):
        return at_inner & (j == tail) & (zz == far_end)

    def used(j):
        if not lend:
            return j >= 0
        return (j != lent) | jnp.logical_not(at_end)

    def lend_x(j, zz):
        for peer in peers:
            for whole in (True, False):

                @pl.when(j == (lent if whole else split))
                def _():
                    begin, size = (0, CHUNK) if whole else (CHUNK, EXTRA)
                    rows = piece(lent, zz, c) if whole else opening(zz, c)
                    pltpu.make_async_remote_copy(
                        src_ref=xbuf.at[rows],
                        dst_ref=lent_x.at[lax.rem(sp, 2), zz, c, pl.ds(begin, size)],
                        send_sem=lent_x_send,
                        recv_sem=lent_x_recv.at[
                            lax.rem(sp, 2), jnp.where(zz == far_end, 1, 0)
                        ],
                        device_id={"sp": peer, "tp": z * 2 + sp // 2},
                        device_id_type=MESH,
                    ).start()

    def w_copy(slot, device, send_sem):
        rows = pl.ds(pl.multiple_of(slot * feats, feats), feats)
        return pltpu.make_async_remote_copy(
            src_ref=lent_w.at[rows],
            dst_ref=lent_w.at[rows],
            send_sem=send_sem,
            recv_sem=lent_w_recv.at[slot],
            device_id={"tp": device},
            device_id_type=MESH,
        )

    def lend_w(slot):
        return w_copy(slot, inner * 2 + c, lent_w_send)

    def pair_w(slot):
        return w_copy(slot, tp + 1 - 2 * c, lent_w_pair)

    def w_copy_all(send_sem):
        return pltpu.make_async_remote_copy(
            src_ref=lent_w,
            dst_ref=lent_w,
            send_sem=send_sem,
            recv_sem=lent_w_recv.at[0],
            device_id={"tp": tp + 1 - 2 * c},
            device_id_type=MESH,
        )

    def given(n):
        both = (sent_tots, lent_terms, sent_reads)[n]
        return pltpu.make_async_remote_copy(
            src_ref=both,
            dst_ref=both,
            send_sem=back_send.at[n],
            recv_sem=back_recv.at[n],
            device_id={"tp": tp + 1 - 2 * c},
            device_id_type=MESH,
        )

    def ask_copy(core):
        return pltpu.make_async_remote_copy(
            src_ref=asks.at[pl.ds(2 * core, 2)],
            dst_ref=asked,
            send_sem=ask_send,
            recv_sem=ask_recv,
            device_id={"tp": inner * 2 + core},
            device_id_type=MESH,
        )

    def hint_copy():
        return pltpu.make_async_remote_copy(
            src_ref=hint,
            dst_ref=hint,
            send_sem=hint_send,
            recv_sem=hint_recv,
            device_id={"tp": end * 2 + c},
            device_id_type=MESH,
        )

    def give_back(n, p):
        lines = pl.ds(2 * c, 2)
        src, dst = (
            (sent_tots.at[p], back_tots.at[lax.rem(sp, 2), lines]),
            (lent_terms.at[p], back_terms.at[lax.rem(sp, 2), lines]),
            (sent_reads.at[p], back_reads.at[lax.rem(sp, 2), c]),
        )[n]
        return pltpu.make_async_remote_copy(
            src_ref=src,
            dst_ref=dst,
            send_sem=back_send.at[n],
            recv_sem=back_recv.at[n],
            device_id={"sp": p, "tp": end * 2 + sp // 2},
            device_id_type=MESH,
        )

    for j in range(chunks):
        own_copy(j).start()
    for load in loads:
        load.start()
    if lend:
        pl.when(lender)(lambda: stage_w(lambda copy: copy.start()))

    barrier = pltpu.get_barrier_semaphore()

    def greet(ahead, device):
        @pl.when(ahead)
        def _():
            pl.semaphore_signal(barrier, inc=1, device_id=device, device_id_type=MESH)

    close = at_end | at_inner if lend else False
    apart = jnp.logical_not(close)
    for way, edge in ((0, 0), (1, n_z - 1)):
        there = z + 2 * way - 1
        met = z != edge
        if lend:
            met = met & jnp.logical_not(close & ((there == end) | (there == inner)))
        greet(met, {"tp": there * 2 + c})
    if lend:
        for p in range(n_sp):
            for plane in (end, inner):
                for core in range(2):
                    known = close & ((p != sp) | (plane != z) | (core != c))
                    greet(known, {"sp": p, "tp": plane * 2 + core})
        greet(apart, {"tp": tp + 1 - 2 * c})
        for peer in peers:
            greet(apart, {"sp": peer})
        far = jnp.where(close, 4 * n_sp - 1 + jnp.where(at_inner, 1, 0), 2 + n_sp)
    else:
        greet(tp >= 0, {"tp": tp + 1 - 2 * c})
        for peer in peers:
            greet(tp >= 0, {"sp": peer})
        far = n_sp + jnp.where(z > 0, 1, 0) + jnp.where(z < n_z - 1, 1, 0)

    acc_k[...] = jnp.zeros_like(acc_k)
    acc_v[...] = jnp.zeros_like(acc_v)
    acc_l[...] = jnp.zeros_like(acc_l)
    acc_s[...] = jnp.zeros_like(acc_s)
    if lend:

        @pl.when(at_inner)
        def _():
            lent_kv[...] = jnp.zeros_like(lent_kv)
            lent_l[...] = jnp.zeros_like(lent_l)
            lent_s[...] = jnp.zeros_like(lent_s)

        @pl.when(jnp.logical_not(at_end))
        def _():
            back_terms[...] = jnp.zeros_like(back_terms)
            back_tots[...] = jnp.zeros_like(back_tots)
            back_reads[...] = jnp.zeros_like(back_reads)

    pl.semaphore_wait(barrier, far)

    def open_chunk(j, _):
        own_copy(j).wait()
        each_way(j, z, lambda copy: copy.start())

        @pl.when(used(j))
        def _():
            each_pair(j, z, c, lambda copy: copy.start())

        return 0

    lax.fori_loop(0, chunks, open_chunk, 0)
    if lend:

        @pl.when(at_inner)
        def _():
            lend_x(split, z)
            lend_x(lent, z)

    for load in loads:
        load.wait()
    if lend:
        pl.when(lender)(lambda: stage_w(lambda copy: copy.wait()))

    def project(scaled, slot, rows, weights, accs):
        deep = pl.ds(pl.multiple_of(slot * feats, feats), feats)
        for weight, acc in zip(weights, accs):
            acc[rows] += jnp.dot(scaled, weight[deep, :], preferred_element_type=F32)

    def reduce_rank(wide, scaled, slot, rows, acc_rank, acc_square):
        deep = pl.ds(pl.multiple_of(slot * feats, feats), feats)
        acc_rank[rows] += lax.dot_general(
            scaled, wd[:, deep], (((1,), (1,)), ((), ())), preferred_element_type=F32
        )
        square = wide * wide
        total = square[:, 0:128]
        for lane in range(128, feats, 128):
            total = total + square[:, lane : lane + 128]
        acc_square[rows] += total

    def skipped(j):
        return jnp.where(at_end & (j == split), EXTRA, 0)

    def add_shard(j, zz, cc):
        slot = zz * 2 + cc
        wide = xbuf[piece(j, zz, cc)].astype(F32)
        if lend:
            row = lax.broadcasted_iota(jnp.int32, wide.shape, 0)
            wide = jnp.where(row >= skipped(j), wide, 0.0)
        scaled = (wide * gain_ref[slot]).astype(BF16)
        project(scaled, slot, j, (wk, wv), (acc_k, acc_v))
        reduce_rank(wide, scaled, slot, j, acc_l, acc_s)

    def source(i):
        away = (i + 1) // 2
        return z + flip * (2 * lax.rem(i, 2) - 1) * away

    def visit(i, j):
        zz = source(i)

        @pl.when(used(j))
        def _():
            @pl.when(i > 0)
            def _():
                each_pair(j, zz, c, lambda copy: copy.wait_recv())
                if lend:

                    @pl.when(jnp.logical_not(held(j, zz)))
                    def _():
                        each_way(j, zz, lambda copy: copy.start())

                else:
                    each_way(j, zz, lambda copy: copy.start())
                each_pair(j, zz, c, lambda copy: copy.start())
                if lend:

                    pl.when(at_inner)(lambda: lend_x(j, zz))

            add_shard(j, zz, c)

    def complete(i, j):
        zz = source(i)

        @pl.when(used(j))
        def _():
            each_pair(j, zz, 1 - c, lambda copy: copy.wait_recv())
            add_shard(j, zz, 1 - c)

    def normed(acc_rank, acc_square, rows):
        inv_rms = lax.rsqrt(jnp.sum(acc_square[rows], axis=1, keepdims=True) / model + 1e-06)
        return acc_rank[rows] * inv_rms, inv_rms

    def faded(low_rank, gate_up, gate_bias, start, skip=None):
        size = low_rank.shape[0]
        gate = gate_bias[...] + jnp.dot(
            jnp.concatenate(split3(low_rank), axis=1),
            jnp.concatenate([gate_up[...]] * 3, axis=0),
            preferred_element_type=F32,
        )
        log_decay = (jnp.minimum(gate, 0.0) - jnp.log1p(jnp.exp(-jnp.abs(gate)))) / 16.0
        if skip is not None:
            row = lax.broadcasted_iota(jnp.int32, log_decay.shape, 0)
            log_decay = jnp.where(row >= skip, log_decay, 0.0)
        later = (
            lax.broadcasted_iota(jnp.int32, (size, size), 1)
            > lax.broadcasted_iota(jnp.int32, (size, size), 0)
        ).astype(BF16)
        suffix = start + jnp.dot(
            jnp.concatenate([later] * 3, axis=1),
            jnp.concatenate(split3(log_decay), axis=0),
            preferred_element_type=F32,
        )
        return jnp.exp(suffix), start + jnp.sum(log_decay, axis=0, keepdims=True)

    def fade_chunk(j, low_rank, inv_rms):
        skip = skipped(j) if lend else None
        weights, total = faded(low_rank, up, bias, carry[...], skip)
        fade[...] = weights
        scale[...] = jnp.broadcast_to(inv_rms, scale.shape)
        carry[...] = total

        @pl.when(lax.rem(j, per_seq) == per_seq - 1)
        def _():
            send_total(j // per_seq)

    def finish_chunk(j):
        seq = j // per_seq

        @pl.when(lax.rem(j, per_seq) == 0)
        def _():
            carry[...] = jnp.zeros_like(carry)
            state[seq] = jnp.zeros(state.shape[1:], F32)

        last = lax.rem(j, per_seq) == per_seq - 1

        @pl.when(used(j))
        def _():
            known = at_end & (j == tail) if lend else j < 0

            @pl.when(jnp.logical_not(known))
            def _():
                fade_chunk(j, *normed(acc_l, acc_s, j))

            inv_rms = scale[:, :1]
            keys = (acc_k[j] * inv_rms).astype(BF16).astype(F32)
            weighted = keys * fade[...]
            values = (acc_v[j] * inv_rms).astype(BF16)
            for h in range(heads):
                part = weighted[:, h * DK : (h + 1) * DK].T.astype(BF16)
                rows = pl.ds(h * DK, DK)
                state[seq, rows, :] = state[seq, rows, :] + jnp.dot(
                    part, values[:, h * DV : (h + 1) * DV], preferred_element_type=F32
                )

        if lend:

            @pl.when(jnp.logical_not(used(j)))
            def _():
                send_total(seq)

        @pl.when(last)
        def _():
            send_terms(seq)

    def tot_copy(seq, peer):
        return pltpu.make_async_remote_copy(
            src_ref=tots.at[seq, sp],
            dst_ref=tots.at[seq, sp],
            send_sem=tot_send.at[seq],
            recv_sem=tot_recv.at[seq],
            device_id={"sp": peer},
            device_id_type=MESH,
        )

    def term_copy(seq, peer):
        return pltpu.make_async_remote_copy(
            src_ref=terms.at[seq, peer],
            dst_ref=landed.at[seq, sp],
            send_sem=term_send.at[seq],
            recv_sem=term_recv.at[seq],
            device_id={"sp": peer},
            device_id_type=MESH,
        )

    def read_copy(seq, peer):
        return pltpu.make_async_remote_copy(
            src_ref=reads.at[seq, sp],
            dst_ref=reads.at[seq, sp],
            send_sem=read_send.at[seq],
            recv_sem=read_recv.at[seq],
            device_id={"sp": peer},
            device_id_type=MESH,
        )

    def others(ref, seq, sems):
        return pltpu.make_async_remote_copy(
            src_ref=ref.at[seq, pl.ds(0, n_sp - 1)],
            dst_ref=ref.at[seq, pl.ds(0, n_sp - 1)],
            send_sem=sems[0].at[seq],
            recv_sem=sems[1].at[seq],
            device_id={"sp": peers[0]},
            device_id_type=MESH,
        )

    def all_tots(seq):
        return others(tots, seq, (tot_send, tot_recv))

    def all_terms(seq):
        return others(landed, seq, (term_send, term_recv))

    def all_reads(seq):
        return others(reads, seq, (read_send, read_recv))

    def send_total(seq):
        tots[seq, sp] = carry[...]
        for peer in peers:
            tot_copy(seq, peer).start()

    def send_terms(seq):
        for h in range(heads):
            for p in range(n_sp):
                row = h * DK + p * share
                terms[seq, p, h] = state[seq, row : row + share, :].astype(BF16)
        for peer in peers:
            term_copy(seq, peer).start()

    def back_copy(n):
        both = (back_tots, back_terms, back_reads)[n]
        return pltpu.make_async_remote_copy(
            src_ref=both,
            dst_ref=both,
            send_sem=back_send.at[n],
            recv_sem=back_recv.at[n],
            device_id={"tp": inner * 2 + c},
            device_id_type=MESH,
        )

    def column(row, begin, size):
        chosen = (
            lax.broadcasted_iota(jnp.int32, (size, DK), 0) + begin
            == lax.broadcasted_iota(jnp.int32, (size, DK), 1)
        )
        return jnp.sum(jnp.where(chosen, row, 0.0), axis=1, keepdims=True)

    def query(seq, h):
        return query_ref[seq : seq + 1, h * DK : (h + 1) * DK].astype(F32)

    def send_parts(seq):
        loaned = lend and seq == LENT_SEQ
        if loaned:
            pl.when(jnp.logical_not(at_end))(lambda: all_tots(seq).wait_recv())
        else:
            all_tots(seq).wait_recv()
        for h in range(heads):
            after = jnp.zeros((1, DK), F32)
            for p in range(n_sp):
                total = tots[seq, p][:, h * DK : (h + 1) * DK]
                if loaned:
                    total = total + back_tots[h, p]
                after = after + jnp.where(p > sp, total, 0.0)
            wanted = column(query(seq, h) * jnp.exp(after), 0, DK)
            reads[seq, sp, h : h + 1, :] = jnp.sum(
                wanted * state[seq, h * DK : (h + 1) * DK, :], axis=0, keepdims=True
            )
        for peer in peers:
            read_copy(seq, peer).start()

    def send_asks():
        all_tots(LENT_SEQ).wait_recv()
        back_copy(0).wait_recv()

        def chosen(rows):
            picked = rows[0]
            for h in range(1, heads):
                picked = jnp.where(lax.rem(sp, 2) == h, rows[h], picked)
            return picked

        after = jnp.zeros((1, DK), F32)
        asker = chosen([query(LENT_SEQ, h) for h in range(heads)])
        for p in reversed(range(n_sp)):
            kept = [tots[LENT_SEQ, p][:, h * DK : (h + 1) * DK] for h in range(heads)]
            after = after + chosen(kept)
            asks[p] = asker * jnp.exp(after)
            after = after + chosen([back_tots[h, p] for h in range(heads)])

        @pl.when(lender)
        def _():
            for core in range(2):
                ask_copy(core).start()

    def sum_terms(seq, loaned):
        after = [jnp.zeros((1, DK), F32)] * heads
        factors = [None] * n_sp
        back_factors = [None] * n_sp
        for p in reversed(range(n_sp)):
            factors[p] = [column(jnp.exp(row), sp * share, share) for row in after]
            after = [after[h] + tots[seq, p][:, h * DK : (h + 1) * DK] for h in range(heads)]
            if loaned:
                back_factors[p] = [column(jnp.exp(row), sp * share, share) for row in after]
                after = [after[h] + back_tots[h, p] for h in range(heads)]
        all_terms(seq).wait_recv()
        if loaned:
            pl.when(at_end)(lambda: back_copy(1).wait_recv())
        for h in range(heads):
            own = state[seq, pl.ds(pl.multiple_of(h * DK + sp * share, share), share), :]
            total = jnp.zeros((share, DV), F32)
            for p in range(n_sp):
                block = jnp.where(p == sp, own, landed[seq, p, h].astype(F32))
                total = total + factors[p][h] * block
                if loaned:
                    total = total + back_factors[p][h] * back_terms[h, p].astype(F32)
            cache_ref[seq, h] = total.astype(BF16)

    def give_read(seq):
        all_reads(seq).wait_recv()
        parts_ref[seq] = reads[seq]
        if lend and seq == LENT_SEQ:
            pl.when(at_end)(lambda: back_copy(2).wait_recv())
            for h in range(heads):
                parts_ref[seq, 0, h : h + 1] = (
                    reads[seq, 0, h : h + 1] + back_reads[h, 0] + back_reads[h, 1]
                )

    def lent_scaled(slot):
        wide = lent_x[:, slot // 2, lax.rem(slot, 2)].reshape(2 * lent_rows, feats).astype(F32)
        return wide, (wide * gain_ref[slot]).astype(BF16)

    lent_blocks = [slice(line * lent_rows, (line + 1) * lent_rows) for line in range(2)]
    every = slice(None)

    def collect(slot, _):
        zz, cc = slot // 2, lax.rem(slot, 2)
        for line in range(2):

            @pl.when(2 * c + line == sp)
            def _():
                lent_x[line, zz, cc, :CHUNK] = xbuf[piece(lent, zz, cc)]
                lent_x[line, zz, cc, CHUNK:] = xbuf[opening(zz, cc)]

        wide, scaled = lent_scaled(slot)
        reduce_rank(wide, scaled, slot, every, lent_l, lent_s)
        return 0

    def await_lent(far):
        begin, size = (far_end, 1) if far else (jnp.where(low_half, 0, 1), n_z - 1)
        for line in range(2):

            @pl.when(2 * c + line != sp)
            def _():
                pltpu.make_async_remote_copy(
                    src_ref=lent_x.at[line, pl.ds(begin, size)],
                    dst_ref=lent_x.at[line, pl.ds(begin, size)],
                    send_sem=lent_x_send,
                    recv_sem=lent_x_recv.at[line, int(far)],
                    device_id={"tp": tp + 1 - 2 * c},
                    device_id_type=MESH,
                ).wait_recv()

    def collect_near(part):
        pl.when(part == 0)(lambda: await_lent(False))
        for cc in range(2):
            collect((jnp.where(low_half, 0, 1) + part) * 2 + cc, 0)

    def prepare_lent():
        await_lent(True)
        for cc in range(2):
            collect(far_end * 2 + cc, 0)
        for line, rows in enumerate(lent_blocks):
            low_rank, inv_rms = normed(lent_l, lent_s, rows)
            weights, total = faded(low_rank, lent_up, lent_bias, jnp.zeros((1, DK), F32))
            lent_fade[rows] = weights
            lent_scale[rows] = jnp.broadcast_to(inv_rms, weights.shape)
            for q in range(n_sp):
                sent_tots[q, line] = total
        for p in range(n_sp):
            give_back(0, p).start()

    def work_off():
        @pl.when(c == sp // 2)
        def _():
            for slot in range(relayed, slots - 1):
                pair_w(slot).wait_recv()
                pair_w(slot).start()

        def multiply(slot, _):
            @pl.when((c != sp // 2) | (slot == slots - 1))
            def _():
                pair_w(slot).wait_recv()

            @pl.when((c == sp // 2) & (slot == slots - 1))
            def _():
                pair_w(slot).start()

            _, scaled = lent_scaled(slot)
            project(scaled, slot, every, (lent_w,), (lent_kv,))
            return 0

        lax.fori_loop(0, slots, multiply, 0)
        for line, rows in enumerate(lent_blocks):
            inv_rms = lent_scale[rows, :1]
            keys = (lent_kv[rows, :DK] * inv_rms).astype(BF16).astype(F32)
            weighted = keys * lent_fade[rows]
            values = (lent_kv[rows, DK:] * inv_rms).astype(BF16)
            block = jnp.dot(weighted.T.astype(BF16), values, preferred_element_type=F32)
            for p in range(n_sp):
                lent_terms[p, line] = block[p * share : (p + 1) * share].astype(BF16)
            lent_state[line] = block
        for p in range(n_sp):
            give_back(1, p).start()
        ask_copy(c).wait_recv()
        heard = jnp.zeros((1, DV), F32)
        for line in range(2):
            wanted = column(asked[line], 0, DK)
            heard = heard + jnp.sum(wanted * lent_state[line], axis=0, keepdims=True)
        for p in range(n_sp):
            sent_reads[p] = heard
        for p in range(n_sp):
            give_back(2, p).start()

    def send_hint():
        low_rank, inv_rms = normed(acc_l, acc_s, tail)
        spread = jnp.broadcast_to(inv_rms, (CHUNK, 128 - low_rank.shape[1]))
        hint[...] = jnp.concatenate([low_rank, spread], axis=1).T[: hint.shape[0]]
        hint_copy().start()

        each_way(tail, far_end, lambda copy: copy.start())

    def take_hint():
        hint_copy().wait_recv()
        rank = wd.shape[0]
        full = jnp.concatenate(
            [hint[...], jnp.zeros((128 - hint.shape[0], CHUNK), F32)], axis=0
        ).T
        fade_chunk(tail, full[:, :rank], full[:, rank : rank + 1])
        send_asks()

    steps = 2 * n_z - 2

    def ready(i, j):
        zz = source(i)
        return (zz >= 0) & (zz < n_z)

    def settle(i, j):
        final = i == final_step
        closing = final & (j == tail)

        @pl.when(ready(i, j))
        def _():
            complete(i, j)
            if lend:
                pl.when(at_inner & closing)(send_hint)

            @pl.when(final)
            def _():
                finish_chunk(j)

    def step(t, _):
        i, j = t // chunks, lax.rem(t, chunks)
        last_i, last_j = (t - 1) // chunks, lax.rem(t - 1, chunks)
        early = at_end & (i == final_step) & (j == tail) if lend else t < 0
        if lend:

            @pl.when(early)
            def _():
                settle(last_i, last_j)
                take_hint()

            due = (2 * j + 1) // 3
            relaying = at_inner & (c == sp // 2) & (i == final_step) & ((3 * due + 1) // 2 == j)

            @pl.when(relaying & (due < relayed))
            def _():
                pair_w(due).wait_recv()
                pair_w(due).start()

            @pl.when(lender & (t == 2 * chunks))
            def _():
                def lend_slot(slot, _):
                    lend_w(slot).start()
                    return 0

                lax.fori_loop(0, slots, lend_slot, 0)

        if lend:
            pl.when(at_inner & (i == final_step) & (j == tail))(prepare_lent)
            part = j - (tail - n_z + 1)
            pl.when(at_inner & (i == final_step) & (part >= 0) & (j < tail))(
                lambda: collect_near(part)
            )

        @pl.when(ready(i, j))
        def _():
            visit(i, j)

        @pl.when(jnp.logical_not(early))
        def _():
            settle(last_i, last_j)

        return 0

    visit(0, 0)
    lax.fori_loop(1, steps * chunks, step, 0)
    settle(steps - 1, chunks - 1)
    if lend:

        @pl.when(at_inner)
        def _():
            work_off()

    for seq in range(seqs):
        send_parts(seq)
    for seq in range(seqs):
        sum_terms(seq, lend and seq == LENT_SEQ)

    def drained(count, send_sem):
        pltpu.make_async_remote_copy(
            src_ref=xbuf.at[pl.ds(0, count)],
            dst_ref=xbuf.at[pl.ds(0, count)],
            send_sem=send_sem,
            recv_sem=recv.at[0, 0, 0],
            device_id={"tp": tp + 1 - 2 * c},
            device_id_type=MESH,
        ).wait_send()

    for plane in range(n_z):
        edge = plane in (0, n_z - 1)
        hops = (0 if plane == 0 else n_z - plane) + (0 if plane == n_z - 1 else plane + 1)
        hops = hops * chunks * CHUNK
        pairs = n_z * chunks * CHUNK
        if lend and plane in (1, n_z - 2):
            hops -= (n_z - 1) * lent_rows
        if lend and edge:
            pairs -= n_z * lent_rows

        @pl.when(z == plane)
        def _():
            drained(hops, hop_send)
            drained(pairs, pair_send)

    if lend:

        @pl.when(lender)
        def _():
            w_copy_all(lent_w_send).wait_send()
            pltpu.make_async_remote_copy(
                src_ref=asks,
                dst_ref=asks,
                send_sem=ask_send,
                recv_sem=ask_recv,
                device_id={"tp": inner * 2 + c},
                device_id_type=MESH,
            ).wait_send()

        @pl.when(at_inner)
        def _():
            pl.when(c == sp // 2)(lambda: w_copy_all(lent_w_pair).wait_send())
            drained(n_z * (n_sp - 1) * lent_rows, lent_x_send)
            given(0).wait_send()
            given(1).wait_send()
            given(2).wait_send()
            hint_copy().wait_send()

    for seq in range(seqs):
        give_read(seq)
    for seq in range(seqs):
        for kind in (all_tots, all_terms, all_reads):
            kind(seq).wait_send()


def norm_kernel(cache_in, parts_ref, gain_ref, cache_ref, read_ref):
    cache_ref[...] = cache_in[...]
    seqs, n_sp, heads, _ = parts_ref.shape
    for seq in range(seqs):
        readout = parts_ref[seq, 0]
        for p in range(1, n_sp):
            readout = readout + parts_ref[seq, p]
        mean = jnp.mean(readout * readout, axis=-1, keepdims=True)
        normed = (readout * lax.rsqrt(mean + 1e-06) * gain_ref[...]).astype(BF16)
        for h in range(heads):
            read_ref[seq : seq + 1, h * DV : (h + 1) * DV] = normed[h : h + 1, :]


def per_device(
    n_sp,
    n_z,
    inputs,
    in_gain,
    key_weight,
    value_weight,
    decay_down,
    decay_up,
    decay_bias,
    new_query,
    out_gain,
):
    seqs, span, feats = inputs.shape
    model, key_cols = key_weight.shape
    value_cols = value_weight.shape[1]
    rank = decay_down.shape[1]
    heads = key_cols // DK
    chunks = seqs * (span // CHUNK)
    share = DK // n_sp
    slots = 2 * n_z
    vmem = pl.BlockSpec(memory_space=pltpu.VMEM)
    hbm = pl.BlockSpec(memory_space=pl.ANY)
    dma = pltpu.SemaphoreType.DMA
    lent = []
    if lends(n_sp, n_z, heads):
        lent = [
            pltpu.VMEM((2, n_z, 2, CHUNK + EXTRA, feats), BF16),
            pltpu.VMEM((model, DK + DV), BF16),
            pltpu.VMEM((rank, DK), BF16),
            pltpu.VMEM((1, DK), F32),
            pltpu.VMEM((2 * (CHUNK + EXTRA), DK + DV), F32),
            pltpu.VMEM((2 * (CHUNK + EXTRA), rank), F32),
            pltpu.VMEM((2 * (CHUNK + EXTRA), 128), F32),
            pltpu.VMEM((2 * (CHUNK + EXTRA), DK), F32),
            pltpu.VMEM((2 * (CHUNK + EXTRA), DK), F32),
            pltpu.VMEM((rank + 8, CHUNK), F32),
            pltpu.VMEM((n_sp, 2, share, DV), BF16),
            pltpu.VMEM((n_sp, 2, 1, DK), F32),
            pltpu.VMEM((heads, n_sp, share, DV), BF16),
            pltpu.VMEM((heads, n_sp, 1, DK), F32),
            pltpu.VMEM((n_sp, 1, DK), F32),
            pltpu.VMEM((2, 1, DK), F32),
            pltpu.VMEM((n_sp, 1, DV), F32),
            pltpu.VMEM((heads, 2, 1, DV), F32),
            pltpu.VMEM((2, DK, DV), F32),
            dma,
            dma,
            dma,
            dma,
            dma,
            dma((2, 2)),
            dma,
            dma,
            dma((slots,)),
            dma((3,)),
            dma((3,)),
        ]
    cache, parts = pl.pallas_call(
        functools.partial(kernel, n_sp, n_z),
        out_shape=(
            jax.ShapeDtypeStruct((seqs, heads, share, DV), BF16),
            jax.ShapeDtypeStruct((seqs, n_sp, heads, DV), F32),
        ),
        in_specs=[hbm] * 8,
        out_specs=(vmem, vmem),
        scratch_shapes=[
            pltpu.VMEM((chunks * slots * CHUNK, feats), BF16),
            pltpu.VMEM((model, key_cols), BF16),
            pltpu.VMEM((model, value_cols), BF16),
            pltpu.VMEM((rank, model), BF16),
            pltpu.VMEM((rank, key_cols), BF16),
            pltpu.VMEM((1, key_cols), F32),
            pltpu.VMEM((slots, 1, feats), F32),
            pltpu.VMEM((seqs, key_cols), BF16),
            pltpu.VMEM((chunks, CHUNK, key_cols), F32),
            pltpu.VMEM((chunks, CHUNK, value_cols), F32),
            pltpu.VMEM((chunks, CHUNK, rank), F32),
            pltpu.VMEM((chunks, CHUNK, 128), F32),
            pltpu.VMEM((seqs, key_cols, DV), F32),
            pltpu.VMEM((1, key_cols), F32),
            pltpu.VMEM((CHUNK, key_cols), F32),
            pltpu.VMEM((CHUNK, 128), F32),
            pltpu.VMEM((seqs, n_sp, 1, key_cols), F32),
            pltpu.VMEM((seqs, n_sp, heads, share, DV), BF16),
            pltpu.VMEM((seqs, n_sp, heads, share, DV), BF16),
            pltpu.VMEM((seqs, n_sp, heads, DV), F32),
            dma((11,)),
            dma((chunks,)),
            dma,
            dma,
            dma((chunks, n_z, 2)),
            dma((seqs,)),
            dma((seqs,)),
            dma((seqs,)),
            dma((seqs,)),
            dma((seqs,)),
            dma((seqs,)),
        ]
        + lent,
        compiler_params=pltpu.CompilerParams(
            collective_id=0, has_side_effects=True, vmem_limit_bytes=60 * 1024 * 1024
        ),
    )(
        inputs,
        in_gain.reshape(slots, 1, feats),
        key_weight,
        value_weight,
        decay_down.T,
        decay_up,
        decay_bias.reshape(1, -1),
        new_query,
    )
    return pl.pallas_call(
        norm_kernel,
        out_shape=(
            jax.ShapeDtypeStruct((seqs, heads, share, DV), BF16),
            jax.ShapeDtypeStruct((seqs, heads * DV), BF16),
        ),
        in_specs=[vmem, vmem, vmem],
        out_specs=(vmem, vmem),
    )(cache, parts, out_gain.reshape(1, -1))


def solution(mesh):
    in_specs = (
        P(None, "sp", "tp"),
        P(),
        P(None, "tp"),
        P(None, "tp"),
        P(),
        P(),
        P(),
        P(None, "tp"),
        P(),
    )
    out_specs = (P(None, "tp", "sp", None), P(None, "tp"))
    return jax.shard_map(
        functools.partial(per_device, mesh.shape["sp"], mesh.shape["tp"] // 2),
        mesh=mesh,
        in_specs=in_specs,
        out_specs=out_specs,
        check_vma=False,
    )
```

```python
import functools

import jax
import jax.numpy as jnp
from jax import lax
from jax.experimental import pallas as pl
from jax.experimental.pallas import tpu as pltpu
from jax.sharding import PartitionSpec as P

DK = 128
DV = 256
CHUNK = 128
LENT_SEQ = 0
EXTRA = 64
MESH = pl.DeviceIdType.MESH
F32 = jnp.float32
BF16 = jnp.bfloat16


def split3(value):
    high = value.astype(BF16)
    rest = value - high.astype(F32)
    middle = rest.astype(BF16)
    low = (rest - middle.astype(F32)).astype(BF16)
    return high, middle, low


def lends(n_sp, n_z, heads):
    return n_z >= 4 and n_sp == 2 * heads


def kernel(
    n_sp,
    n_z,
    x_ref,
    gain_hbm,
    wk_hbm,
    wv_hbm,
    wd_hbm,
    up_hbm,
    bias_hbm,
    query_hbm,
    cache_ref,
    parts_ref,
    xbuf,
    wk,
    wv,
    wd,
    up,
    bias,
    gain_ref,
    query_ref,
    acc_k,
    acc_v,
    acc_l,
    acc_s,
    state,
    carry,
    fade,
    scale,
    tots,
    terms,
    landed,
    reads,
    load_sem,
    own_sem,
    hop_send,
    pair_send,
    recv,
    tot_send,
    tot_recv,
    term_send,
    term_recv,
    read_send,
    read_recv,
    lent_x=None,
    lent_w=None,
    lent_up=None,
    lent_bias=None,
    lent_kv=None,
    lent_l=None,
    lent_s=None,
    lent_fade=None,
    lent_scale=None,
    hint=None,
    lent_terms=None,
    sent_tots=None,
    back_terms=None,
    back_tots=None,
    asks=None,
    asked=None,
    sent_reads=None,
    back_reads=None,
    lent_state=None,
    ask_send=None,
    ask_recv=None,
    hint_send=None,
    hint_recv=None,
    lent_x_send=None,
    lent_x_recv=None,
    lent_w_send=None,
    lent_w_pair=None,
    lent_w_recv=None,
    back_send=None,
    back_recv=None,
):
    seqs, span, feats = x_ref.shape
    per_seq = span // CHUNK
    chunks = seqs * per_seq
    heads = wk_hbm.shape[1] // DK
    share = DK // n_sp
    slots = 2 * n_z
    model = slots * feats
    lend = lends(n_sp, n_z, heads)
    lent = LENT_SEQ * per_seq + per_seq - 1
    tail = chunks - 1
    split = lent - 1
    lent_rows = CHUNK + EXTRA
    relayed = min(slots - 2, chunks // 2 + 1)
    sp = lax.axis_index("sp")
    tp = lax.axis_index("tp")
    z = tp // 2
    c = lax.rem(tp, 2)
    key_cols = heads * DK
    at_end = (z == 0) | (z == n_z - 1)
    low_half = z < n_z // 2
    end = jnp.where(low_half, 0, n_z - 1)
    inner = jnp.where(low_half, 1, n_z - 2)
    at_inner = z == inner
    far_end = n_z - 1 - end
    flip = jnp.where(low_half, 1, -1)
    reach = jnp.where(low_half, n_z - 1 - z, z)
    final_step = 2 * reach - 1
    lender = at_end & (c == sp // 2)
    peers = [lax.rem(sp + off, n_sp) for off in range(1, n_sp)]

    first = pl.multiple_of(tp * key_cols, key_cols)
    loads = [
        pltpu.make_async_copy(wk_hbm, wk, load_sem.at[0]),
        pltpu.make_async_copy(wv_hbm, wv, load_sem.at[1]),
        pltpu.make_async_copy(wd_hbm, wd, load_sem.at[2]),
        pltpu.make_async_copy(up_hbm.at[:, pl.ds(first, key_cols)], up, load_sem.at[3]),
        pltpu.make_async_copy(bias_hbm.at[:, pl.ds(first, key_cols)], bias, load_sem.at[4]),
        pltpu.make_async_copy(gain_hbm, gain_ref, load_sem.at[5]),
        pltpu.make_async_copy(query_hbm, query_ref, load_sem.at[6]),
    ]
    if lend:
        other = pl.multiple_of((end * 2 * heads + sp) * DK, DK)
        loads += [
            pltpu.make_async_copy(up_hbm.at[:, pl.ds(other, DK)], lent_up, load_sem.at[7]),
            pltpu.make_async_copy(bias_hbm.at[:, pl.ds(other, DK)], lent_bias, load_sem.at[8]),
        ]

    def stage_w(act):
        head = lax.rem(sp, 2)
        for n, (src, width, begin) in enumerate(((wk_hbm, DK, 0), (wv_hbm, DV, DK))):
            columns = pl.ds(pl.multiple_of(head * width, width), width)
            dst = lent_w.at[:, begin : begin + width]
            act(pltpu.make_async_copy(src.at[:, columns], dst, load_sem.at[9 + n]))

    def piece(j, zz, cc, skip=0):
        start = ((j * n_z + zz) * 2 + cc) * CHUNK + skip
        return pl.ds(pl.multiple_of(start, 16), CHUNK - skip)

    def opening(zz, cc):
        start = ((split * n_z + zz) * 2 + cc) * CHUNK
        return pl.ds(pl.multiple_of(start, 16), EXTRA)

    def chunk_rows(j):
        seq = j // per_seq
        start = (per_seq - 1 - lax.rem(j, per_seq)) * CHUNK
        return seq, pl.multiple_of(start, CHUNK)

    def own_copy(j):
        seq, start = chunk_rows(j)
        return pltpu.make_async_copy(
            x_ref.at[seq, pl.ds(start, CHUNK), :], xbuf.at[piece(j, z, c)], own_sem.at[j]
        )

    def hop_copy(j, zz, way, skip=0):
        return pltpu.make_async_remote_copy(
            src_ref=xbuf.at[piece(j, zz, c, skip)],
            dst_ref=xbuf.at[piece(j, zz, c, skip)],
            send_sem=hop_send,
            recv_sem=recv.at[j, zz, c],
            device_id={"tp": (z + 2 * way - 1) * 2 + c},
            device_id_type=MESH,
        )

    def pair_copy(j, zz, cc, skip=0):
        return pltpu.make_async_remote_copy(
            src_ref=xbuf.at[piece(j, zz, cc, skip)],
            dst_ref=xbuf.at[piece(j, zz, cc, skip)],
            send_sem=pair_send,
            recv_sem=recv.at[j, zz, cc],
            device_id={"tp": tp + 1 - 2 * c},
            device_id_type=MESH,
        )

    def each_pair(j, zz, cc, act):
        if not lend:
            act(pair_copy(j, zz, cc))
            return
        short = at_end & (j == split)
        pl.when(short)(lambda: act(pair_copy(j, zz, cc, EXTRA)))
        pl.when(jnp.logical_not(short))(lambda: act(pair_copy(j, zz, cc)))

    def each_way(j, zz, act):
        for way, edge in ((0, 0), (1, n_z - 1)):
            there = z + 2 * way - 1
            beyond = (zz >= z) if way == 0 else (zz <= z)
            wanted = (z != edge) & beyond
            if lend:
                short = (j == split) & (there == edge)
                pl.when(wanted & short)(lambda: act(hop_copy(j, zz, way, EXTRA)))
                wanted = wanted & jnp.logical_not(short) & ((j != lent) | (there != edge))
            pl.when(wanted)(lambda: act(hop_copy(j, zz, way)))

    def held(j, zz):
        return at_inner & (j == tail) & (zz == far_end)

    def used(j):
        if not lend:
            return j >= 0
        return (j != lent) | jnp.logical_not(at_end)

    def lend_x(j, zz):
        for peer in peers:
            for whole in (True, False):

                @pl.when(j == (lent if whole else split))
                def _():
                    begin, size = (0, CHUNK) if whole else (CHUNK, EXTRA)
                    rows = piece(lent, zz, c) if whole else opening(zz, c)
                    pltpu.make_async_remote_copy(
                        src_ref=xbuf.at[rows],
                        dst_ref=lent_x.at[lax.rem(sp, 2), zz, c, pl.ds(begin, size)],
                        send_sem=lent_x_send,
                        recv_sem=lent_x_recv.at[
                            lax.rem(sp, 2), jnp.where(zz == far_end, 1, 0)
                        ],
                        device_id={"sp": peer, "tp": z * 2 + sp // 2},
                        device_id_type=MESH,
                    ).start()

    def w_copy(slot, device, send_sem):
        rows = pl.ds(pl.multiple_of(slot * feats, feats), feats)
        return pltpu.make_async_remote_copy(
            src_ref=lent_w.at[rows],
            dst_ref=lent_w.at[rows],
            send_sem=send_sem,
            recv_sem=lent_w_recv.at[slot],
            device_id={"tp": device},
            device_id_type=MESH,
        )

    def lend_w(slot):
        return w_copy(slot, inner * 2 + c, lent_w_send)

    def pair_w(slot):
        return w_copy(slot, tp + 1 - 2 * c, lent_w_pair)

    def w_copy_all(send_sem):
        return pltpu.make_async_remote_copy(
            src_ref=lent_w,
            dst_ref=lent_w,
            send_sem=send_sem,
            recv_sem=lent_w_recv.at[0],
            device_id={"tp": tp + 1 - 2 * c},
            device_id_type=MESH,
        )

    def given(n):
        both = (sent_tots, lent_terms, sent_reads)[n]
        return pltpu.make_async_remote_copy(
            src_ref=both,
            dst_ref=both,
            send_sem=back_send.at[n],
            recv_sem=back_recv.at[n],
            device_id={"tp": tp + 1 - 2 * c},
            device_id_type=MESH,
        )

    def ask_copy(core):
        return pltpu.make_async_remote_copy(
            src_ref=asks.at[pl.ds(2 * core, 2)],
            dst_ref=asked,
            send_sem=ask_send,
            recv_sem=ask_recv,
            device_id={"tp": inner * 2 + core},
            device_id_type=MESH,
        )

    def hint_copy():
        return pltpu.make_async_remote_copy(
            src_ref=hint,
            dst_ref=hint,
            send_sem=hint_send,
            recv_sem=hint_recv,
            device_id={"tp": end * 2 + c},
            device_id_type=MESH,
        )

    def give_back(n, p):
        lines = pl.ds(2 * c, 2)
        src, dst = (
            (sent_tots.at[p], back_tots.at[lax.rem(sp, 2), lines]),
            (lent_terms.at[p], back_terms.at[lax.rem(sp, 2), lines]),
            (sent_reads.at[p], back_reads.at[lax.rem(sp, 2), c]),
        )[n]
        return pltpu.make_async_remote_copy(
            src_ref=src,
            dst_ref=dst,
            send_sem=back_send.at[n],
            recv_sem=back_recv.at[n],
            device_id={"sp": p, "tp": end * 2 + sp // 2},
            device_id_type=MESH,
        )

    for j in range(chunks):
        own_copy(j).start()
    for load in loads:
        load.start()
    if lend:
        pl.when(lender)(lambda: stage_w(lambda copy: copy.start()))

    barrier = pltpu.get_barrier_semaphore()

    def greet(ahead, device):
        @pl.when(ahead)
        def _():
            pl.semaphore_signal(barrier, inc=1, device_id=device, device_id_type=MESH)

    close = at_end | at_inner if lend else False
    apart = jnp.logical_not(close)
    for way, edge in ((0, 0), (1, n_z - 1)):
        there = z + 2 * way - 1
        met = z != edge
        if lend:
            met = met & jnp.logical_not(close & ((there == end) | (there == inner)))
        greet(met, {"tp": there * 2 + c})
    if lend:
        for p in range(n_sp):
            for plane in (end, inner):
                for core in range(2):
                    known = close & ((p != sp) | (plane != z) | (core != c))
                    greet(known, {"sp": p, "tp": plane * 2 + core})
        greet(apart, {"tp": tp + 1 - 2 * c})
        for peer in peers:
            greet(apart, {"sp": peer})
        far = jnp.where(close, 4 * n_sp - 1 + jnp.where(at_inner, 1, 0), 2 + n_sp)
    else:
        greet(tp >= 0, {"tp": tp + 1 - 2 * c})
        for peer in peers:
            greet(tp >= 0, {"sp": peer})
        far = n_sp + jnp.where(z > 0, 1, 0) + jnp.where(z < n_z - 1, 1, 0)

    acc_k[...] = jnp.zeros_like(acc_k)
    acc_v[...] = jnp.zeros_like(acc_v)
    acc_l[...] = jnp.zeros_like(acc_l)
    acc_s[...] = jnp.zeros_like(acc_s)
    if lend:

        @pl.when(at_inner)
        def _():
            lent_kv[...] = jnp.zeros_like(lent_kv)
            lent_l[...] = jnp.zeros_like(lent_l)
            lent_s[...] = jnp.zeros_like(lent_s)

        @pl.when(jnp.logical_not(at_end))
        def _():
            back_terms[...] = jnp.zeros_like(back_terms)
            back_tots[...] = jnp.zeros_like(back_tots)
            back_reads[...] = jnp.zeros_like(back_reads)

    pl.semaphore_wait(barrier, far)

    def open_chunk(j, _):
        own_copy(j).wait()
        each_way(j, z, lambda copy: copy.start())

        @pl.when(used(j))
        def _():
            each_pair(j, z, c, lambda copy: copy.start())

        return 0

    lax.fori_loop(0, chunks, open_chunk, 0)
    if lend:

        @pl.when(at_inner)
        def _():
            lend_x(split, z)
            lend_x(lent, z)

    for load in loads:
        load.wait()
    if lend:
        pl.when(lender)(lambda: stage_w(lambda copy: copy.wait()))

    def project(scaled, slot, rows, weights, accs):
        deep = pl.ds(pl.multiple_of(slot * feats, feats), feats)
        for weight, acc in zip(weights, accs):
            acc[rows] += jnp.dot(scaled, weight[deep, :], preferred_element_type=F32)

    def reduce_rank(wide, scaled, slot, rows, acc_rank, acc_square):
        deep = pl.ds(pl.multiple_of(slot * feats, feats), feats)
        acc_rank[rows] += lax.dot_general(
            scaled, wd[:, deep], (((1,), (1,)), ((), ())), preferred_element_type=F32
        )
        square = wide * wide
        total = square[:, 0:128]
        for lane in range(128, feats, 128):
            total = total + square[:, lane : lane + 128]
        acc_square[rows] += total

    def skipped(j):
        return jnp.where(at_end & (j == split), EXTRA, 0)

    def add_shard(j, zz, cc):
        slot = zz * 2 + cc
        wide = xbuf[piece(j, zz, cc)].astype(F32)
        if lend:
            row = lax.broadcasted_iota(jnp.int32, wide.shape, 0)
            wide = jnp.where(row >= skipped(j), wide, 0.0)
        scaled = (wide * gain_ref[slot]).astype(BF16)
        project(scaled, slot, j, (wk, wv), (acc_k, acc_v))
        reduce_rank(wide, scaled, slot, j, acc_l, acc_s)

    def source(i):
        away = (i + 1) // 2
        return z + flip * (2 * lax.rem(i, 2) - 1) * away

    def visit(i, j):
        zz = source(i)

        @pl.when(used(j))
        def _():
            @pl.when(i > 0)
            def _():
                each_pair(j, zz, c, lambda copy: copy.wait_recv())
                if lend:

                    @pl.when(jnp.logical_not(held(j, zz)))
                    def _():
                        each_way(j, zz, lambda copy: copy.start())

                else:
                    each_way(j, zz, lambda copy: copy.start())
                each_pair(j, zz, c, lambda copy: copy.start())
                if lend:

                    pl.when(at_inner)(lambda: lend_x(j, zz))

            add_shard(j, zz, c)

    def complete(i, j):
        zz = source(i)

        @pl.when(used(j))
        def _():
            each_pair(j, zz, 1 - c, lambda copy: copy.wait_recv())
            add_shard(j, zz, 1 - c)

    def normed(acc_rank, acc_square, rows):
        inv_rms = lax.rsqrt(jnp.sum(acc_square[rows], axis=1, keepdims=True) / model + 1e-06)
        return acc_rank[rows] * inv_rms, inv_rms

    def faded(low_rank, gate_up, gate_bias, start, skip=None):
        size = low_rank.shape[0]
        gate = gate_bias[...] + jnp.dot(
            jnp.concatenate(split3(low_rank), axis=1),
            jnp.concatenate([gate_up[...]] * 3, axis=0),
            preferred_element_type=F32,
        )
        log_decay = (jnp.minimum(gate, 0.0) - jnp.log1p(jnp.exp(-jnp.abs(gate)))) / 16.0
        if skip is not None:
            row = lax.broadcasted_iota(jnp.int32, log_decay.shape, 0)
            log_decay = jnp.where(row >= skip, log_decay, 0.0)
        later = (
            lax.broadcasted_iota(jnp.int32, (size, size), 1)
            > lax.broadcasted_iota(jnp.int32, (size, size), 0)
        ).astype(BF16)
        suffix = start + jnp.dot(
            jnp.concatenate([later] * 3, axis=1),
            jnp.concatenate(split3(log_decay), axis=0),
            preferred_element_type=F32,
        )
        return jnp.exp(suffix), start + jnp.sum(log_decay, axis=0, keepdims=True)

    def fade_chunk(j, low_rank, inv_rms):
        skip = skipped(j) if lend else None
        weights, total = faded(low_rank, up, bias, carry[...], skip)
        fade[lax.rem(j, 2)] = weights
        scale[lax.rem(j, 2)] = jnp.broadcast_to(inv_rms, scale.shape[1:])
        carry[...] = total

        @pl.when(lax.rem(j, per_seq) == per_seq - 1)
        def _():
            send_total(j // per_seq)

    def fade_piece(j):
        seq = j // per_seq

        @pl.when(lax.rem(j, per_seq) == 0)
        def _():
            carry[...] = jnp.zeros_like(carry)
            state[seq] = jnp.zeros(state.shape[1:], F32)

        known = at_end & (j == tail) if lend else j < 0

        @pl.when(used(j) & jnp.logical_not(known))
        def _():
            fade_chunk(j, *normed(acc_l, acc_s, j))

        if lend:

            @pl.when(jnp.logical_not(used(j)))
            def _():
                send_total(seq)

    def gather_state(j):
        seq = j // per_seq

        @pl.when(used(j))
        def _():
            inv_rms = scale[lax.rem(j, 2)][:, :1]
            keys = (acc_k[j] * inv_rms).astype(BF16).astype(F32)
            weighted = keys * fade[lax.rem(j, 2)]
            values = (acc_v[j] * inv_rms).astype(BF16)
            for h in range(heads):
                part = weighted[:, h * DK : (h + 1) * DK].T.astype(BF16)
                rows = pl.ds(h * DK, DK)
                state[seq, rows, :] = state[seq, rows, :] + jnp.dot(
                    part, values[:, h * DV : (h + 1) * DV], preferred_element_type=F32
                )

        @pl.when(lax.rem(j, per_seq) == per_seq - 1)
        def _():
            send_terms(seq)

    def tot_copy(seq, peer):
        return pltpu.make_async_remote_copy(
            src_ref=tots.at[seq, sp],
            dst_ref=tots.at[seq, sp],
            send_sem=tot_send.at[seq],
            recv_sem=tot_recv.at[seq],
            device_id={"sp": peer},
            device_id_type=MESH,
        )

    def term_copy(seq, peer):
        return pltpu.make_async_remote_copy(
            src_ref=terms.at[seq, peer],
            dst_ref=landed.at[seq, sp],
            send_sem=term_send.at[seq],
            recv_sem=term_recv.at[seq],
            device_id={"sp": peer},
            device_id_type=MESH,
        )

    def read_copy(seq, peer):
        return pltpu.make_async_remote_copy(
            src_ref=reads.at[seq, sp],
            dst_ref=reads.at[seq, sp],
            send_sem=read_send.at[seq],
            recv_sem=read_recv.at[seq],
            device_id={"sp": peer},
            device_id_type=MESH,
        )

    def others(ref, seq, sems):
        return pltpu.make_async_remote_copy(
            src_ref=ref.at[seq, pl.ds(0, n_sp - 1)],
            dst_ref=ref.at[seq, pl.ds(0, n_sp - 1)],
            send_sem=sems[0].at[seq],
            recv_sem=sems[1].at[seq],
            device_id={"sp": peers[0]},
            device_id_type=MESH,
        )

    def all_tots(seq):
        return others(tots, seq, (tot_send, tot_recv))

    def all_terms(seq):
        return others(landed, seq, (term_send, term_recv))

    def all_reads(seq):
        return others(reads, seq, (read_send, read_recv))

    def send_total(seq):
        tots[seq, sp] = carry[...]
        for peer in peers:
            tot_copy(seq, peer).start()

    def send_terms(seq):
        for h in range(heads):
            for p in range(n_sp):
                row = h * DK + p * share
                terms[seq, p, h] = state[seq, row : row + share, :].astype(BF16)
        for peer in peers:
            term_copy(seq, peer).start()

    def back_copy(n):
        both = (back_tots, back_terms, back_reads)[n]
        return pltpu.make_async_remote_copy(
            src_ref=both,
            dst_ref=both,
            send_sem=back_send.at[n],
            recv_sem=back_recv.at[n],
            device_id={"tp": inner * 2 + c},
            device_id_type=MESH,
        )

    def column(row, begin, size):
        chosen = (
            lax.broadcasted_iota(jnp.int32, (size, DK), 0) + begin
            == lax.broadcasted_iota(jnp.int32, (size, DK), 1)
        )
        return jnp.sum(jnp.where(chosen, row, 0.0), axis=1, keepdims=True)

    def query(seq, h):
        return query_ref[seq : seq + 1, h * DK : (h + 1) * DK].astype(F32)

    def send_parts(seq):
        loaned = lend and seq == LENT_SEQ
        if loaned:
            pl.when(jnp.logical_not(at_end))(lambda: all_tots(seq).wait_recv())
        else:
            all_tots(seq).wait_recv()
        for h in range(heads):
            after = jnp.zeros((1, DK), F32)
            for p in range(n_sp):
                total = tots[seq, p][:, h * DK : (h + 1) * DK]
                if loaned:
                    total = total + back_tots[h, p]
                after = after + jnp.where(p > sp, total, 0.0)
            wanted = column(query(seq, h) * jnp.exp(after), 0, DK)
            reads[seq, sp, h : h + 1, :] = jnp.sum(
                wanted * state[seq, h * DK : (h + 1) * DK, :], axis=0, keepdims=True
            )
        for peer in peers:
            read_copy(seq, peer).start()

    def send_asks():
        all_tots(LENT_SEQ).wait_recv()
        back_copy(0).wait_recv()

        def chosen(rows):
            picked = rows[0]
            for h in range(1, heads):
                picked = jnp.where(lax.rem(sp, 2) == h, rows[h], picked)
            return picked

        after = jnp.zeros((1, DK), F32)
        asker = chosen([query(LENT_SEQ, h) for h in range(heads)])
        for p in reversed(range(n_sp)):
            kept = [tots[LENT_SEQ, p][:, h * DK : (h + 1) * DK] for h in range(heads)]
            after = after + chosen(kept)
            asks[p] = asker * jnp.exp(after)
            after = after + chosen([back_tots[h, p] for h in range(heads)])

        @pl.when(lender)
        def _():
            for core in range(2):
                ask_copy(core).start()

    def sum_terms(seq, loaned):
        after = [jnp.zeros((1, DK), F32)] * heads
        factors = [None] * n_sp
        back_factors = [None] * n_sp
        for p in reversed(range(n_sp)):
            factors[p] = [column(jnp.exp(row), sp * share, share) for row in after]
            after = [after[h] + tots[seq, p][:, h * DK : (h + 1) * DK] for h in range(heads)]
            if loaned:
                back_factors[p] = [column(jnp.exp(row), sp * share, share) for row in after]
                after = [after[h] + back_tots[h, p] for h in range(heads)]
        all_terms(seq).wait_recv()
        if loaned:
            pl.when(at_end)(lambda: back_copy(1).wait_recv())
        for h in range(heads):
            own = state[seq, pl.ds(pl.multiple_of(h * DK + sp * share, share), share), :]
            total = jnp.zeros((share, DV), F32)
            for p in range(n_sp):
                block = jnp.where(p == sp, own, landed[seq, p, h].astype(F32))
                total = total + factors[p][h] * block
                if loaned:
                    total = total + back_factors[p][h] * back_terms[h, p].astype(F32)
            cache_ref[seq, h] = total.astype(BF16)

    def give_read(seq):
        all_reads(seq).wait_recv()
        parts_ref[seq] = reads[seq]
        if lend and seq == LENT_SEQ:
            pl.when(at_end)(lambda: back_copy(2).wait_recv())
            for h in range(heads):
                parts_ref[seq, 0, h : h + 1] = (
                    reads[seq, 0, h : h + 1] + back_reads[h, 0] + back_reads[h, 1]
                )

    def lent_scaled(slot):
        wide = lent_x[:, slot // 2, lax.rem(slot, 2)].reshape(2 * lent_rows, feats).astype(F32)
        return wide, (wide * gain_ref[slot]).astype(BF16)

    lent_blocks = [slice(line * lent_rows, (line + 1) * lent_rows) for line in range(2)]
    every = slice(None)

    def collect(slot, _):
        zz, cc = slot // 2, lax.rem(slot, 2)
        for line in range(2):

            @pl.when(2 * c + line == sp)
            def _():
                lent_x[line, zz, cc, :CHUNK] = xbuf[piece(lent, zz, cc)]
                lent_x[line, zz, cc, CHUNK:] = xbuf[opening(zz, cc)]

        wide, scaled = lent_scaled(slot)
        reduce_rank(wide, scaled, slot, every, lent_l, lent_s)
        return 0

    def await_lent(far):
        begin, size = (far_end, 1) if far else (jnp.where(low_half, 0, 1), n_z - 1)
        for line in range(2):

            @pl.when(2 * c + line != sp)
            def _():
                pltpu.make_async_remote_copy(
                    src_ref=lent_x.at[line, pl.ds(begin, size)],
                    dst_ref=lent_x.at[line, pl.ds(begin, size)],
                    send_sem=lent_x_send,
                    recv_sem=lent_x_recv.at[line, int(far)],
                    device_id={"tp": tp + 1 - 2 * c},
                    device_id_type=MESH,
                ).wait_recv()

    def collect_near(part):
        pl.when(part == 0)(lambda: await_lent(False))
        for cc in range(2):
            collect((jnp.where(low_half, 0, 1) + part) * 2 + cc, 0)

    def prepare_lent():
        await_lent(True)
        for cc in range(2):
            collect(far_end * 2 + cc, 0)
        for line, rows in enumerate(lent_blocks):
            low_rank, inv_rms = normed(lent_l, lent_s, rows)
            weights, total = faded(low_rank, lent_up, lent_bias, jnp.zeros((1, DK), F32))
            lent_fade[rows] = weights
            lent_scale[rows] = jnp.broadcast_to(inv_rms, weights.shape)
            for q in range(n_sp):
                sent_tots[q, line] = total
        for p in range(n_sp):
            give_back(0, p).start()

    def work_off():
        @pl.when(c == sp // 2)
        def _():
            for slot in range(relayed, slots - 1):
                pair_w(slot).wait_recv()
                pair_w(slot).start()

        def multiply(slot, _):
            @pl.when((c != sp // 2) | (slot == slots - 1))
            def _():
                pair_w(slot).wait_recv()

            @pl.when((c == sp // 2) & (slot == slots - 1))
            def _():
                pair_w(slot).start()

            _, scaled = lent_scaled(slot)
            project(scaled, slot, every, (lent_w,), (lent_kv,))
            return 0

        lax.fori_loop(0, slots, multiply, 0)
        for line, rows in enumerate(lent_blocks):
            inv_rms = lent_scale[rows, :1]
            keys = (lent_kv[rows, :DK] * inv_rms).astype(BF16).astype(F32)
            weighted = keys * lent_fade[rows]
            values = (lent_kv[rows, DK:] * inv_rms).astype(BF16)
            block = jnp.dot(weighted.T.astype(BF16), values, preferred_element_type=F32)
            for p in range(n_sp):
                lent_terms[p, line] = block[p * share : (p + 1) * share].astype(BF16)
            lent_state[line] = block
        for p in range(n_sp):
            give_back(1, p).start()
        ask_copy(c).wait_recv()
        heard = jnp.zeros((1, DV), F32)
        for line in range(2):
            wanted = column(asked[line], 0, DK)
            heard = heard + jnp.sum(wanted * lent_state[line], axis=0, keepdims=True)
        for p in range(n_sp):
            sent_reads[p] = heard
        for p in range(n_sp):
            give_back(2, p).start()

    def send_hint():
        low_rank, inv_rms = normed(acc_l, acc_s, tail)
        spread = jnp.broadcast_to(inv_rms, (CHUNK, 128 - low_rank.shape[1]))
        hint[...] = jnp.concatenate([low_rank, spread], axis=1).T[: hint.shape[0]]
        hint_copy().start()

        each_way(tail, far_end, lambda copy: copy.start())

    def take_hint():
        hint_copy().wait_recv()
        rank = wd.shape[0]
        full = jnp.concatenate(
            [hint[...], jnp.zeros((128 - hint.shape[0], CHUNK), F32)], axis=0
        ).T
        fade_chunk(tail, full[:, :rank], full[:, rank : rank + 1])
        send_asks()

    steps = 2 * n_z - 2

    def ready(i, j):
        zz = source(i)
        return (zz >= 0) & (zz < n_z)

    def settle(i, j, whole=True):
        final = i == final_step
        closing = final & (j == tail)

        @pl.when(ready(i, j))
        def _():
            complete(i, j)
            if lend:
                pl.when(at_inner & closing)(send_hint)

            @pl.when(final)
            def _():
                fade_piece(j)
                if whole:
                    gather_state(j)

    def step(t, _):
        i, j = t // chunks, lax.rem(t, chunks)
        last_i, last_j = (t - 1) // chunks, lax.rem(t - 1, chunks)
        early = at_end & (i == final_step) & (j == tail) if lend else t < 0
        if lend:

            @pl.when(early)
            def _():
                settle(last_i, last_j, False)
                take_hint()
                gather_state(last_j)

            due = (2 * j + 1) // 3
            relaying = at_inner & (c == sp // 2) & (i == final_step) & ((3 * due + 1) // 2 == j)

            @pl.when(relaying & (due < relayed))
            def _():
                pair_w(due).wait_recv()
                pair_w(due).start()

            @pl.when(lender & (t == 2 * chunks))
            def _():
                def lend_slot(slot, _):
                    lend_w(slot).start()
                    return 0

                lax.fori_loop(0, slots, lend_slot, 0)

        if lend:
            pl.when(at_inner & (i == final_step) & (j == tail))(prepare_lent)
            part = j - (tail - n_z + 1)
            pl.when(at_inner & (i == final_step) & (part >= 0) & (j < tail))(
                lambda: collect_near(part)
            )

        @pl.when(ready(i, j))
        def _():
            visit(i, j)

        @pl.when(jnp.logical_not(early))
        def _():
            settle(last_i, last_j)

        return 0

    visit(0, 0)
    lax.fori_loop(1, steps * chunks, step, 0)
    settle(steps - 1, chunks - 1)
    if lend:

        @pl.when(at_inner)
        def _():
            work_off()

    for seq in range(seqs):
        send_parts(seq)
    for seq in range(seqs):
        sum_terms(seq, lend and seq == LENT_SEQ)

    def drained(count, send_sem):
        pltpu.make_async_remote_copy(
            src_ref=xbuf.at[pl.ds(0, count)],
            dst_ref=xbuf.at[pl.ds(0, count)],
            send_sem=send_sem,
            recv_sem=recv.at[0, 0, 0],
            device_id={"tp": tp + 1 - 2 * c},
            device_id_type=MESH,
        ).wait_send()

    for plane in range(n_z):
        edge = plane in (0, n_z - 1)
        hops = (0 if plane == 0 else n_z - plane) + (0 if plane == n_z - 1 else plane + 1)
        hops = hops * chunks * CHUNK
        pairs = n_z * chunks * CHUNK
        if lend and plane in (1, n_z - 2):
            hops -= (n_z - 1) * lent_rows
        if lend and edge:
            pairs -= n_z * lent_rows

        @pl.when(z == plane)
        def _():
            drained(hops, hop_send)
            drained(pairs, pair_send)

    if lend:

        @pl.when(lender)
        def _():
            w_copy_all(lent_w_send).wait_send()
            pltpu.make_async_remote_copy(
                src_ref=asks,
                dst_ref=asks,
                send_sem=ask_send,
                recv_sem=ask_recv,
                device_id={"tp": inner * 2 + c},
                device_id_type=MESH,
            ).wait_send()

        @pl.when(at_inner)
        def _():
            pl.when(c == sp // 2)(lambda: w_copy_all(lent_w_pair).wait_send())
            drained(n_z * (n_sp - 1) * lent_rows, lent_x_send)
            given(0).wait_send()
            given(1).wait_send()
            given(2).wait_send()
            hint_copy().wait_send()

    for seq in range(seqs):
        give_read(seq)
    for seq in range(seqs):
        for kind in (all_tots, all_terms, all_reads):
            kind(seq).wait_send()


def norm_kernel(cache_in, parts_ref, gain_ref, cache_ref, read_ref):
    cache_ref[...] = cache_in[...]
    seqs, n_sp, heads, _ = parts_ref.shape
    for seq in range(seqs):
        readout = parts_ref[seq, 0]
        for p in range(1, n_sp):
            readout = readout + parts_ref[seq, p]
        mean = jnp.mean(readout * readout, axis=-1, keepdims=True)
        normed = (readout * lax.rsqrt(mean + 1e-06) * gain_ref[...]).astype(BF16)
        for h in range(heads):
            read_ref[seq : seq + 1, h * DV : (h + 1) * DV] = normed[h : h + 1, :]


def per_device(
    n_sp,
    n_z,
    inputs,
    in_gain,
    key_weight,
    value_weight,
    decay_down,
    decay_up,
    decay_bias,
    new_query,
    out_gain,
):
    seqs, span, feats = inputs.shape
    model, key_cols = key_weight.shape
    value_cols = value_weight.shape[1]
    rank = decay_down.shape[1]
    heads = key_cols // DK
    chunks = seqs * (span // CHUNK)
    share = DK // n_sp
    slots = 2 * n_z
    vmem = pl.BlockSpec(memory_space=pltpu.VMEM)
    hbm = pl.BlockSpec(memory_space=pl.ANY)
    dma = pltpu.SemaphoreType.DMA
    lent = []
    if lends(n_sp, n_z, heads):
        lent = [
            pltpu.VMEM((2, n_z, 2, CHUNK + EXTRA, feats), BF16),
            pltpu.VMEM((model, DK + DV), BF16),
            pltpu.VMEM((rank, DK), BF16),
            pltpu.VMEM((1, DK), F32),
            pltpu.VMEM((2 * (CHUNK + EXTRA), DK + DV), F32),
            pltpu.VMEM((2 * (CHUNK + EXTRA), rank), F32),
            pltpu.VMEM((2 * (CHUNK + EXTRA), 128), F32),
            pltpu.VMEM((2 * (CHUNK + EXTRA), DK), F32),
            pltpu.VMEM((2 * (CHUNK + EXTRA), DK), F32),
            pltpu.VMEM((rank + 8, CHUNK), F32),
            pltpu.VMEM((n_sp, 2, share, DV), BF16),
            pltpu.VMEM((n_sp, 2, 1, DK), F32),
            pltpu.VMEM((heads, n_sp, share, DV), BF16),
            pltpu.VMEM((heads, n_sp, 1, DK), F32),
            pltpu.VMEM((n_sp, 1, DK), F32),
            pltpu.VMEM((2, 1, DK), F32),
            pltpu.VMEM((n_sp, 1, DV), F32),
            pltpu.VMEM((heads, 2, 1, DV), F32),
            pltpu.VMEM((2, DK, DV), F32),
            dma,
            dma,
            dma,
            dma,
            dma,
            dma((2, 2)),
            dma,
            dma,
            dma((slots,)),
            dma((3,)),
            dma((3,)),
        ]
    cache, parts = pl.pallas_call(
        functools.partial(kernel, n_sp, n_z),
        out_shape=(
            jax.ShapeDtypeStruct((seqs, heads, share, DV), BF16),
            jax.ShapeDtypeStruct((seqs, n_sp, heads, DV), F32),
        ),
        in_specs=[hbm] * 8,
        out_specs=(vmem, vmem),
        scratch_shapes=[
            pltpu.VMEM((chunks * slots * CHUNK, feats), BF16),
            pltpu.VMEM((model, key_cols), BF16),
            pltpu.VMEM((model, value_cols), BF16),
            pltpu.VMEM((rank, model), BF16),
            pltpu.VMEM((rank, key_cols), BF16),
            pltpu.VMEM((1, key_cols), F32),
            pltpu.VMEM((slots, 1, feats), F32),
            pltpu.VMEM((seqs, key_cols), BF16),
            pltpu.VMEM((chunks, CHUNK, key_cols), F32),
            pltpu.VMEM((chunks, CHUNK, value_cols), F32),
            pltpu.VMEM((chunks, CHUNK, rank), F32),
            pltpu.VMEM((chunks, CHUNK, 128), F32),
            pltpu.VMEM((seqs, key_cols, DV), F32),
            pltpu.VMEM((1, key_cols), F32),
            pltpu.VMEM((2, CHUNK, key_cols), F32),
            pltpu.VMEM((2, CHUNK, 128), F32),
            pltpu.VMEM((seqs, n_sp, 1, key_cols), F32),
            pltpu.VMEM((seqs, n_sp, heads, share, DV), BF16),
            pltpu.VMEM((seqs, n_sp, heads, share, DV), BF16),
            pltpu.VMEM((seqs, n_sp, heads, DV), F32),
            dma((11,)),
            dma((chunks,)),
            dma,
            dma,
            dma((chunks, n_z, 2)),
            dma((seqs,)),
            dma((seqs,)),
            dma((seqs,)),
            dma((seqs,)),
            dma((seqs,)),
            dma((seqs,)),
        ]
        + lent,
        compiler_params=pltpu.CompilerParams(
            collective_id=0, has_side_effects=True, vmem_limit_bytes=60 * 1024 * 1024
        ),
    )(
        inputs,
        in_gain.reshape(slots, 1, feats),
        key_weight,
        value_weight,
        decay_down.T,
        decay_up,
        decay_bias.reshape(1, -1),
        new_query,
    )
    return pl.pallas_call(
        norm_kernel,
        out_shape=(
            jax.ShapeDtypeStruct((seqs, heads, share, DV), BF16),
            jax.ShapeDtypeStruct((seqs, heads * DV), BF16),
        ),
        in_specs=[vmem, vmem, vmem],
        out_specs=(vmem, vmem),
    )(cache, parts, out_gain.reshape(1, -1))


def solution(mesh):
    in_specs = (
        P(None, "sp", "tp"),
        P(),
        P(None, "tp"),
        P(None, "tp"),
        P(),
        P(),
        P(),
        P(None, "tp"),
        P(),
    )
    out_specs = (P(None, "tp", "sp", None), P(None, "tp"))
    return jax.shard_map(
        functools.partial(per_device, mesh.shape["sp"], mesh.shape["tp"] // 2),
        mesh=mesh,
        in_specs=in_specs,
        out_specs=out_specs,
        check_vma=False,
    )
```
